256 devices in a mesh: ep: 64 (over z, y, core), tp: 4 (over x).
Axes of the slice: x: 4, y: 4, z: 8, core: 2. Of those that a mesh axis runs over, the one named last changes fastest.
Arguments:
- queries: bfloat16 [16384, 8, 128], P('ep', 'tp'), may hold values from -6 to 6
- keys: bfloat16 [16384, 4, 128], P('ep', 'tp'), may hold values from -6 to 6
- values: bfloat16 [16384, 4, 128], P('ep', 'tp'), may hold values from -6 to 6
- query_gain: float32 [128], replicated, may hold values from 1.5 to 7
- key_gain: float32 [128], replicated, may hold values from 1.5 to 7
- routed_rows: bfloat16 [32768, 2048], P(('ep', 'tp')), may hold values from -6 to 6
- mixture_gain: float32 [2048], replicated, may hold values from 0.1 to 1.9
- expert_index: int32 [32768, 2], P(('ep', 'tp')), may hold values from 0 to 63, as said below
- route_weights: float32 [32768, 2], P(('ep', 'tp')), may hold values from 0.1 to 1
- expert_gate: bfloat16 [64, 768, 2048], P('ep', 'tp'), may hold values from -0.125 to 0.125
- expert_up: bfloat16 [64, 768, 2048], P('ep', 'tp'), may hold values from -0.125 to 0.125
- expert_down: bfloat16 [64, 768, 2048], P('ep', 'tp'), may hold values from -0.21875 to 0.21875
Outputs:
- attended: bfloat16 [16384, 8, 128], P('ep', 'tp')
- combined: bfloat16 [32768, 2048], P(('ep', 'tp'))
The draws below stay inside these ranges and needn't reach their ends.
Inputs may be any that keep to these rules, and one draw needn't show every extreme that they name: `expert_index`: each row names 2 different experts that lie in one group of 16 consecutive experts. In every aligned block of 128 rows (the rows of one device) no expert is named by more than 8 rows, and the experts of one group, the same group in all blocks, are each named by exactly 8 rows.
All inputs are finite; a program needn't handle non-finite values.
Results may differ from the reference program's by a relative error of at most 0.011.
The reference program's roundings to bfloat16 on the way count: a program that leaves them out, or rounds other values in their place, can miss the bound.
Values may be sent and summed in bfloat16 or wider, within the bound.
A program may use at most 128 MiB of HBM per device.

```python
import jax
import jax.numpy as jnp
from jax import lax

D = 2048
DH = 128
HQ = 8
KVH = 4
FE = 768
GROUPS = 4
TOPK = 2
GRID_W = 64
TOK_A = 256
TOK_B = 128
EXPERTS = 64
EPG = 16
CAP = 8
SEQ = 16384
TOKENS_B = 32768
N_EP = 64
N_TP = 4


def attention_pair(base_key):
    key_query, key_other = jax.random.split(jax.random.fold_in(base_key, 11))
    query_draw = jnp.clip(jax.random.normal(key_query, (SEQ, HQ, DH), jnp.float32), -6.0, 6.0)
    key_draw = jnp.clip(jax.random.normal(key_other, (SEQ, KVH, DH), jnp.float32), -6.0, 6.0)
    return (query_draw, key_draw)


def draw_queries(key, part):
    return attention_pair(key)[0].astype(jnp.bfloat16)


def draw_keys(key, part):
    return attention_pair(key)[1].astype(jnp.bfloat16)


def gain_draw(base_key, salt_value):
    sub_key = jax.random.fold_in(base_key, salt_value)
    drawn = jax.random.uniform(sub_key, (DH,), jnp.float32, 1.5, 3.5)
    return drawn


def draw_query_gain(key, part):
    return gain_draw(key, 13)


def draw_key_gain(key, part):
    return gain_draw(key, 17)


def draw_expert_index(key, part):
    blocks = TOKENS_B // TOK_B
    largest = TOK_B // 2
    remainder = TOK_B - largest
    key_busy, key_cuts, key_offset, key_stride, key_perm = jax.random.split(jax.random.fold_in(key, 29), 5)
    busiest = jax.random.randint(key_busy, (), 0, GROUPS)
    cut_points = jax.random.randint(key_cuts, (blocks, 2), 0, remainder + 1)
    low_cut = jnp.min(cut_points, axis=1)[:, None]
    high_cut = jnp.max(cut_points, axis=1)[:, None]
    offsets = jax.random.randint(key_offset, (blocks, GROUPS), 0, EPG)
    strides = jax.random.randint(key_stride, (blocks, GROUPS), 1, EPG)
    rank_row = jnp.arange(TOK_B, dtype=jnp.int32)[None, :]
    beyond = rank_row - largest
    in_busy = rank_row < largest
    which_other = jnp.where(beyond < low_cut, 0, jnp.where(beyond < high_cut, 1, 2))
    begins = jnp.where(which_other == 0, 0, jnp.where(which_other == 1, low_cut, high_cut))
    within = jnp.where(in_busy, rank_row, beyond - begins)
    groups_of = jnp.where(in_busy, busiest, (busiest + 1 + which_other) % GROUPS)
    shift_one = jnp.take_along_axis(offsets, groups_of, axis=1)
    shift_two = jnp.take_along_axis(strides, groups_of, axis=1)
    first_pick = groups_of * EPG + (within + shift_one) % EPG
    second_pick = groups_of * EPG + (within + shift_one + shift_two) % EPG
    pick_table = jnp.stack([first_pick, second_pick], axis=-1)
    orders = jax.vmap(lambda sub_key: jax.random.permutation(sub_key, TOK_B))(jax.random.split(key_perm, blocks))
    shuffled = jnp.take_along_axis(pick_table, orders[:, :, None], axis=1)
    return shuffled.reshape(TOKENS_B, 2).astype(jnp.int32)


def steps_of(own_key, shape, cuts, smallest, high):
    loudness = 1.0
    for dim, shards_of in cuts:
        steps = jax.random.uniform(jax.random.fold_in(jax.random.fold_in(own_key, 6), dim), (shards_of,), jnp.float32, smallest / len(cuts), high / len(cuts))
        loudness = loudness * jnp.repeat(jnp.exp(steps), shape[dim] // shards_of).reshape((-1,) + (1,) * (len(shape) - 1 - dim))
    return loudness


def noise(key, dims, deviation, most, shards=(), kind=jnp.bfloat16):
    values = deviation * jax.random.normal(key, dims, jnp.float32)
    if shards:
        values = values * steps_of(key, dims, shards, -0.22, 0.18)
    return jnp.clip(values, -most, most).astype(kind)


def setup_inputs(seed: int = 0) -> dict:
    arg_keys = jax.random.split(jax.random.key(seed), 13)
    queries = draw_queries(jax.random.fold_in(arg_keys[12], 71), 0)
    keys = draw_keys(jax.random.fold_in(arg_keys[12], 71), 0)
    values = noise(arg_keys[2], (SEQ, KVH, DH), 1.0, 6.0, ((0, 64), (1, 4)))
    query_gain = draw_query_gain(jax.random.fold_in(arg_keys[12], 71), 0)
    key_gain = draw_key_gain(jax.random.fold_in(arg_keys[12], 71), 0)
    routed_rows = noise(arg_keys[5], (TOKENS_B, D), 1.0, 6.0, ((0, 256),))
    mixture_gain = jnp.clip(1.0 + 0.18 * jax.random.normal(arg_keys[6], (D,), jnp.float32), 0.1, 1.9)
    expert_index = draw_expert_index(jax.random.fold_in(arg_keys[12], 71), 0)
    route_weights = jnp.clip(0.1 + 0.9 * jax.random.uniform(arg_keys[8], (TOKENS_B, TOPK), jnp.float32) ** steps_of(arg_keys[8], (TOKENS_B, TOPK), ((0, 256),), -0.2, 0.2), 0.1, 1.0)
    expert_gate = noise(arg_keys[9], (EXPERTS, FE, D), D ** -0.5, 0.125, ((0, 64), (1, 4)))
    expert_up = noise(arg_keys[10], (EXPERTS, FE, D), D ** -0.5, 0.125, ((0, 64), (1, 4)))
    expert_down = noise(arg_keys[11], (EXPERTS, FE, D), FE ** -0.5, 0.21875, ((0, 64), (1, 4)))
    return {"queries": queries, "keys": keys, "values": values, "query_gain": query_gain, "key_gain": key_gain, "routed_rows": routed_rows, "mixture_gain": mixture_gain, "expert_index": expert_index, "route_weights": route_weights, "expert_gate": expert_gate, "expert_up": expert_up, "expert_down": expert_down}


epsilon = 1e-06
rotary_base = 10000.0
floor_value = -1e+30

def normalize(inputs, gain_vector):
    values_f = inputs.astype(jnp.float32)
    return values_f * lax.rsqrt(lax.optimization_barrier(jnp.mean(values_f * values_f, axis=-1, keepdims=True)) + epsilon) * gain_vector

def rotate(normed, positions):
    head_width = normed.shape[-1]
    quarter = head_width // 4
    frequency = rotary_base ** (-jnp.arange(quarter, dtype=jnp.float32) / quarter)
    grid_row = (positions // GRID_W).astype(jnp.float32)
    grid_col = (positions % GRID_W).astype(jnp.float32)
    angles = jnp.concatenate([grid_row[:, None] * frequency, grid_col[:, None] * frequency], axis=-1)[:, None, :]
    cosine_table = jnp.cos(angles)
    sine_table = jnp.sin(angles)
    lower_half, upper_half = jnp.split(normed, 2, axis=-1)
    turned = jnp.concatenate([lower_half * cosine_table - upper_half * sine_table, lower_half * sine_table + upper_half * cosine_table], axis=-1)
    return turned.astype(jnp.bfloat16)

def merge_block(running, key_block, grouped, factor):
    maxima, totals, weighted = running
    block_keys, block_values = key_block
    scores = jnp.einsum('tkgd,skd->kgts', grouped, block_keys.astype(jnp.float32)) * factor
    local_max = lax.optimization_barrier(jnp.max(scores, axis=-1))
    shifted = jnp.exp(scores - local_max[..., None])
    block_mass = lax.optimization_barrier(jnp.sum(shifted, axis=-1))
    rounded = lax.optimization_barrier(shifted.astype(jnp.bfloat16))
    block_sum = jnp.einsum('kgts,skd->kgtd', rounded.astype(jnp.float32), block_values.astype(jnp.float32))
    top_max = jnp.maximum(maxima, local_max)
    keep_old = jnp.exp(maxima - top_max)
    keep_new = jnp.exp(local_max - top_max)
    return (top_max, totals * keep_old + block_mass * keep_new, weighted * keep_old[..., None] + block_sum * keep_new[..., None])

def attend(queries, keys, values, query_gain, key_gain):
    positions = jnp.arange(SEQ, dtype=jnp.int32)
    turned_queries = rotate(normalize(queries, query_gain), positions)
    turned_keys = rotate(normalize(keys, key_gain), positions)
    group_size = HQ // KVH
    grouped = turned_queries.reshape(SEQ, KVH, group_size, DH).astype(jnp.float32)
    key_stack = turned_keys.reshape(N_EP, TOK_A, KVH, DH)
    value_stack = values.reshape(N_EP, TOK_A, KVH, DH)
    factor = DH ** (-0.5)
    initial = (jnp.full((KVH, group_size, SEQ), floor_value, jnp.float32), jnp.zeros((KVH, group_size, SEQ), jnp.float32), jnp.zeros((KVH, group_size, SEQ, DH), jnp.float32))

    def one_block(running, key_block):
        return (merge_block(running, key_block, grouped, factor), None)
    final_state, unused = lax.scan(one_block, initial, (key_stack, value_stack))
    maxima, totals, weighted = final_state
    output = (weighted / totals[..., None]).transpose(2, 0, 1, 3).reshape(SEQ, HQ, DH)
    return output.astype(jnp.bfloat16)

def experts_pass(routed_rows, mixture_gain, expert_index, route_weights, expert_gate, expert_up, expert_down):
    normed_rows = normalize(routed_rows, mixture_gain).astype(jnp.bfloat16)
    flat_ids = expert_index.reshape(-1).astype(jnp.int32)
    assigned = flat_ids.shape[0]
    onehot = (flat_ids[:, None] == jnp.arange(EXPERTS, dtype=jnp.int32)[None, :]).astype(jnp.int32)
    earlier = jnp.cumsum(onehot, axis=0) - onehot
    slot_numbers = lax.optimization_barrier(jnp.sum(earlier * onehot, axis=1)).astype(jnp.int32)
    room = TOKENS_B // TOK_B * CAP
    places = (flat_ids * room + slot_numbers).astype(jnp.int32)
    owners = (jnp.arange(assigned, dtype=jnp.int32) // TOPK).astype(jnp.int32)
    source = jnp.full((EXPERTS * room,), TOKENS_B, jnp.int32).at[places].set(owners).reshape(EXPERTS, room)
    weight_table = jnp.zeros((EXPERTS * room,), jnp.float32).at[places].set(route_weights.reshape(-1).astype(jnp.float32)).reshape(EXPERTS, room)
    padded = jnp.concatenate([normed_rows, jnp.zeros((1, D), jnp.bfloat16)], axis=0)
    part_width = FE // N_TP

    def run_expert(running, expert_args):
        rows_index, slot_weights, gate_weight, up_weight, down_weight = expert_args
        taken_rows = padded[rows_index]
        gate_values = jnp.dot(taken_rows, gate_weight.T, preferred_element_type=jnp.float32)
        up_values = jnp.dot(taken_rows, up_weight.T, preferred_element_type=jnp.float32)
        hidden = (jax.nn.silu(gate_values) * up_values).astype(jnp.bfloat16)
        total = jnp.zeros((room, D), jnp.float32)
        for block_index in range(N_TP):
            lower_col = block_index * part_width
            partial_value = jnp.dot(hidden[:, lower_col:lower_col + part_width], down_weight[lower_col:lower_col + part_width, :], preferred_element_type=jnp.float32)
            rounded = lax.optimization_barrier(partial_value.astype(jnp.bfloat16))
            total = total + rounded.astype(jnp.float32)
        result = total.astype(jnp.bfloat16).astype(jnp.float32)
        running = running.at[rows_index].add(result * slot_weights[:, None])
        return (running, None)
    initial = jnp.zeros((TOKENS_B + 1, D), jnp.float32)
    summed, unused = lax.scan(run_expert, initial, (source, weight_table, expert_gate, expert_up, expert_down))
    return summed[:TOKENS_B].astype(jnp.bfloat16)

def reference(queries, keys, values, query_gain, key_gain, routed_rows, mixture_gain, expert_index, route_weights, expert_gate, expert_up, expert_down):
    attended = attend(queries, keys, values, query_gain, key_gain)
    combined = experts_pass(routed_rows, mixture_gain, expert_index, route_weights, expert_gate, expert_up, expert_down)
    return (attended, combined)
```

```python
import functools

import jax
import jax.numpy as jnp
from jax import lax
from jax.experimental import pallas as pl
from jax.experimental.pallas import tpu as pltpu
from jax.sharding import PartitionSpec as P

GROUPS = 4
GRID_W = 64
NZ, NY, NC = 8, 4, 2
CAP = 8
LOG2E = 1.4426950408889634

epsilon = 1e-06
rotary_base = 10000.0
floor_value = -1e30

F32 = jnp.float32
BF16 = jnp.bfloat16


def rms(values_f, gain):
    mean = jnp.mean(values_f * values_f, axis=-1, keepdims=True)
    return values_f * lax.rsqrt(mean + epsilon) * gain


def step_kernel(
    n_tp,
    q_ref, k_ref, v_ref, qg_ref, kg_ref, cos_ref, sin_ref,
    rows_ref, mg_ref, ei_ref, rw_ref, gate_ref, up_ref, down_ref,
    att_ref, comb_ref,
    kv, wbuf, out, arr, arr16, total, res, ret, qt, acc, stat, dmat, place,
    loc_sem, ws_sem, wr_sem, zs_sem, zr_sem, ys_sem, yr_sem, cs_sem, cr_sem,
    ds_sem, dr_sem, rs_sem, rr_sem,
):
    me = lax.axis_index("ep")
    t = lax.axis_index("tp")
    z, y, c = me // (NY * NC), (me // NC) % NY, me % NC
    n_ep = NZ * NY * NC

    def ep_of(zz, yy, cc):
        return zz * (NY * NC) + yy * NC + cc

    def ahead(k):
        dz, dy, dc = k % NZ, (k // NZ) % NY, k // (NZ * NY)
        return ep_of((z + dz) % NZ, (y + dy) % NY, (c + dc) % NC)

    def behind(k):
        dz, dy, dc = k % NZ, (k // NZ) % NY, k // (NZ * NY)
        return ep_of((z + NZ - dz) % NZ, (y + NY - dy) % NY, (c + NC - dc) % NC)

    def remote(src, dst, s_sem, r_sem, ep, tp):
        return pltpu.make_async_remote_copy(
            src_ref=src, dst_ref=dst, send_sem=s_sem, recv_sem=r_sem,
            device_id=(ep, tp), device_id_type=pl.DeviceIdType.MESH,
        )

    t_next, t_prev = (t + 1) % n_tp, (t + n_tp - 1) % n_tp

    barrier = pltpu.get_barrier_semaphore()

    @pl.loop(1, n_ep)
    def _(k):
        pl.semaphore_signal(barrier, inc=1, device_id=(ahead(k), t), device_id_type=pl.DeviceIdType.MESH)

    for peer in (t_next, t_prev):
        pl.semaphore_signal(barrier, inc=1, device_id=(me, peer), device_id_type=pl.DeviceIdType.MESH)

    half = wbuf.shape[2] // 2
    srcs = (gate_ref, up_ref, down_ref)

    def w_local(p):
        return pltpu.make_async_copy(srcs[p].at[0], wbuf.at[t, p], loc_sem.at[p])

    for p in range(3):
        w_local(p).start()

    cosine, sine = cos_ref[...], sin_ref[...]

    def turn(x, gain):
        n = rms(x.astype(F32), gain)
        return (n * cosine + pltpu.roll(n, x.shape[-1] // 2, 1) * sine).astype(BF16)

    length, width = k_ref.shape
    kv[c, y, z, 0:length, :] = turn(k_ref[...], kg_ref[...])
    v_t = v_ref[...].astype(F32).T.astype(BF16)
    for j in range(length // width):
        kv[c, y, z, length + j * width : length + (j + 1) * width, :] = v_t[:, j * width : (j + 1) * width]
    for h in range(q_ref.shape[1] // width):
        turned = turn(q_ref[:, h * width : (h + 1) * width], qg_ref[...])
        qt[:, h * length : (h + 1) * length] = turned.astype(F32).T.astype(BF16)

    rows_here, model = rows_ref.shape
    ids = ei_ref[...]
    lanes = lax.broadcasted_iota(jnp.int32, (rows_here, n_ep), 1)
    hot = [(ids[:, k : k + 1] == lanes).astype(F32) for k in range(2)]
    above = (
        lax.broadcasted_iota(jnp.int32, (rows_here, rows_here), 1)
        < lax.broadcasted_iota(jnp.int32, (rows_here, rows_here), 0)
    ).astype(F32).astype(BF16)
    earlier = jnp.dot(above, (hot[0] + hot[1]).astype(BF16), preferred_element_type=F32)
    slots = lax.broadcasted_iota(jnp.int32, (rows_here, n_ep * CAP), 1).astype(F32)
    picks = []
    for k in range(2):
        at = ids[:, k : k + 1].astype(F32) * CAP + jnp.sum(earlier * hot[k], axis=1, keepdims=True)
        pick = (at == slots).astype(F32)
        place[k] = pick.astype(BF16)
        picks.append(pick)
    dmat[...] = (picks[0] + picks[1]).T.astype(BF16)
    arr16[0:rows_here, :] = rms(rows_ref[...].astype(F32), mg_ref[...]).astype(BF16)

    @pl.loop(0, n_ep * CAP // 128)
    def _(i):
        block = jnp.dot(
            dmat[pl.ds(i * 128, 128), :], arr16[0:rows_here, :], preferred_element_type=F32
        )
        out[pl.ds(i * (128 // CAP), 128 // CAP)] = block.reshape(128 // CAP, CAP, model).astype(BF16)

    pl.semaphore_wait(barrier, n_ep - 1 + 2)

    def w_part(first):
        return pl.ds(0, half) if first else pl.ds(half, half)

    def w_copy(d, stage, p):
        to = t_next if d == 0 else t_prev
        part = w_part((d == 0) != (stage == 1))
        sems = (ws_sem.at[d, stage, p], wr_sem.at[d, stage, p])
        if stage < 2:
            return remote(srcs[p].at[0, part], wbuf.at[t, p, part], *sems, me, to)
        held = t_prev if d == 0 else t_next
        return remote(wbuf.at[held, p, part], wbuf.at[held, p, part], *sems, me, to)

    for stage in range(2):
        for p in range(3):
            for d in range(2):
                w_copy(d, stage, p).start()

    def z_copy(dz):
        return remote(
            kv.at[c, y, z], kv.at[c, y, z], zs_sem.at[dz], zr_sem.at[dz], ep_of((z + dz) % NZ, y, c), t
        )

    for dz in (1, 7, 2, 6, 3, 5, 4):
        z_copy(dz).start()

    def d_copy(k):
        return remote(out.at[ahead(k)], arr.at[k], ds_sem.at[k], dr_sem.at[k], ahead(k), t)

    @pl.loop(1, n_ep)
    def _(k):
        d_copy(k).start()

    own = pltpu.make_async_copy(out.at[me], arr.at[0], ds_sem.at[0])
    own.start()

    zh = NZ // 2

    def y_copy(d, stage):
        to = (y + 1) % NY if d == 0 else (y + NY - 1) % NY
        first = (d == 0) != (stage == 1)
        part = pl.ds(0, zh) if first else pl.ds(zh, zh)
        held = y if stage < 2 else ((y + NY - 1) % NY if d == 0 else (y + 1) % NY)
        piece = kv.at[c, held, part]
        return remote(piece, piece, ys_sem.at[d, stage], yr_sem.at[d, stage], ep_of(z, to, c), t)

    def c_copy(dy):
        piece = kv.at[c, (y + dy) % NY]
        return remote(piece, piece, cs_sem.at[dy], cr_sem.at[dy], ep_of(z, y, (c + 1) % NC), t)

    for dz in (1, 7, 2, 6, 3, 5, 4):
        z_copy(dz).wait_recv()
    for stage in range(2):
        for d in range(2):
            y_copy(d, stage).start()
    c_copy(0).start()

    for d in range(2):
        for p in range(3):
            w_copy(d, 0, p).wait_recv()
            w_copy(d, 2, p).start()
    for d in range(2):
        y_copy(d, 0).wait_recv()
        y_copy(d, 2).start()

    @pl.loop(1, n_ep)
    def _(k):
        d_copy(k).wait_recv()

    own.wait()
    arr_chunk = 128

    @pl.loop(0, n_ep * CAP // arr_chunk)
    def _(i):
        block = arr[pl.ds(i * (arr_chunk // CAP), arr_chunk // CAP)].astype(F32)
        arr16[pl.ds(i * arr_chunk, arr_chunk), :] = block.reshape(arr_chunk, model).astype(BF16)

    for p in range(3):
        w_local(p).wait()

    step = 256
    contract = (((1,), (1,)), ((), ()))

    def expert(q, i):
        at = pl.ds(i * step, step)
        x = arr16[at, :]
        g = lax.dot_general(x, wbuf[q, 0], contract, preferred_element_type=F32)
        u = lax.dot_general(x, wbuf[q, 1], contract, preferred_element_type=F32)
        hidden = (g / (1.0 + jnp.exp(-g)) * u).astype(BF16)
        part = jnp.dot(hidden, wbuf[q, 2], preferred_element_type=F32)
        return at, part.astype(BF16).astype(F32)

    chunks = n_ep * CAP // step

    @pl.loop(0, chunks)
    def _(i):
        at, part = expert(t, i)
        total[at, :] = part

    for d, held in ((0, t_prev), (1, t_next)):
        for p in range(3):
            w_copy(d, 1, p).wait_recv()

        @pl.loop(0, chunks)
        def _(i):
            at, part = expert(held, i)
            total[at, :] = total[at, :] + part

    for d in range(2):
        for p in range(3):
            w_copy(d, 2, p).wait_recv()

    def r_copy(k):
        return remote(res.at[k], ret.at[me], rs_sem.at[k], rr_sem.at[k], behind(k), t)

    def r_wait(k):
        return remote(res.at[k], ret.at[ahead(k)], rs_sem.at[k], rr_sem.at[k], behind(k), t)

    last = (t + 2) % n_tp
    per = step // CAP

    @pl.loop(0, chunks)
    def _(i):
        at, part = expert(last, i)
        block = (total[at, :] + part).astype(BF16).astype(F32)
        res[pl.ds(i * per, per)] = block.reshape(per, CAP, model).astype(BF16)

    @pl.loop(1, n_ep)
    def _(k):
        r_copy(k).start()

    mine = pltpu.make_async_copy(res.at[0], ret.at[me], rs_sem.at[0])
    mine.start()

    for d in range(2):
        y_copy(d, 1).wait_recv()
    c_copy(1).start()
    c_copy(3).start()
    for d in range(2):
        y_copy(d, 2).wait_recv()
    c_copy(2).start()
    for dy in range(NY):
        c_copy(dy).wait_recv()

    cols = qt.shape[1]
    factor = width ** (-0.5) * LOG2E
    stat[0:1, :] = jnp.full((1, cols), floor_value, F32)
    stat[1:2, :] = jnp.zeros((1, cols), F32)
    acc[...] = jnp.zeros_like(acc)

    def one_block(b):
        cc, yy, zz = b // (NY * NZ), (b // NZ) % NY, b % NZ
        k_block = kv[cc, yy, zz, 0:length, :]
        v_block = jnp.concatenate(
            [kv[cc, yy, zz, length + j * width : length + (j + 1) * width, :] for j in range(length // width)],
            axis=1,
        )
        s = jnp.dot(k_block, qt[...], preferred_element_type=F32)
        m_b = jnp.max(s, axis=0, keepdims=True)
        p = jnp.exp2((s - m_b) * factor)
        l_b = jnp.sum(p, axis=0, keepdims=True)
        a_b = jnp.dot(v_block, p.astype(BF16), preferred_element_type=F32)
        return m_b, l_b, a_b

    @pl.loop(0, NZ * NY * NC // 2)
    def _(b):
        m_0, l_0, a_0 = one_block(2 * b)
        m_1, l_1, a_1 = one_block(2 * b + 1)
        m_old = stat[0:1, :]
        top = jnp.maximum(jnp.maximum(m_0, m_1), m_old)
        keep = jnp.exp2((m_old - top) * factor)
        n_0 = jnp.exp2((m_0 - top) * factor)
        n_1 = jnp.exp2((m_1 - top) * factor)
        stat[0:1, :] = top
        stat[1:2, :] = stat[1:2, :] * keep + l_0 * n_0 + l_1 * n_1
        acc[...] = acc[...] * keep + a_0 * n_0 + a_1 * n_1

    done = acc[...] / stat[1:2, :]
    for h in range(cols // length):
        att_ref[:, h * width : (h + 1) * width] = done[:, h * length : (h + 1) * length].T.astype(BF16)

    @pl.loop(1, n_ep)
    def _(k):
        r_wait(k).wait_recv()

    mine.wait()

    @pl.loop(0, n_ep * CAP // arr_chunk)
    def _(i):
        block = ret[pl.ds(i * (arr_chunk // CAP), arr_chunk // CAP)].astype(F32)
        arr16[pl.ds(i * arr_chunk, arr_chunk), :] = block.reshape(arr_chunk, model).astype(BF16)

    weights = rw_ref[...]
    wide = 512
    for j in range(model // wide):
        block = arr16[:, j * wide : (j + 1) * wide]
        picked = [jnp.dot(place[k], block, preferred_element_type=F32) * weights[:, k : k + 1] for k in range(2)]
        comb_ref[:, j * wide : (j + 1) * wide] = (picked[0] + picked[1]).astype(BF16)

    for stage in range(3):
        for p in range(3):
            for d in range(2):
                w_copy(d, stage, p).wait_send()
        for d in range(2):
            y_copy(d, stage).wait_send()
    for dz in range(1, NZ):
        z_copy(dz).wait_send()
    for dy in range(NY):
        c_copy(dy).wait_send()

    @pl.loop(1, n_ep)
    def _(k):
        d_copy(k).wait_send()
        r_copy(k).wait_send()


def on_device(
    queries, keys, values, query_gain, key_gain, routed_rows, mixture_gain,
    expert_index, route_weights, expert_gate, expert_up, expert_down,
):
    length, heads, width = queries.shape
    rows_here, model = routed_rows.shape
    n_tp = lax.axis_size("tp")
    n_ep = lax.axis_size("ep")
    slots = n_ep * CAP
    part = expert_gate.shape[1]
    positions = lax.axis_index("ep") * length + jnp.arange(length, dtype=jnp.int32)
    quarter = width // 4
    frequency = rotary_base ** (-jnp.arange(quarter, dtype=F32) / quarter)
    grid_row = (positions // GRID_W).astype(F32)
    grid_col = (positions % GRID_W).astype(F32)
    angles = jnp.concatenate([grid_row[:, None] * frequency, grid_col[:, None] * frequency], axis=-1)
    cosine, sine = jnp.cos(angles), jnp.sin(angles)
    cosine = jnp.concatenate([cosine, cosine], axis=-1)
    sine = jnp.concatenate([-sine, sine], axis=-1)
    vmem = pl.BlockSpec(memory_space=pltpu.VMEM)
    hbm = pl.BlockSpec(memory_space=pl.ANY)
    dma = pltpu.SemaphoreType.DMA
    attended, combined = pl.pallas_call(
        functools.partial(step_kernel, n_tp),
        name="step",
        out_shape=(
            jax.ShapeDtypeStruct((length, heads * width), BF16),
            jax.ShapeDtypeStruct((rows_here, model), BF16),
        ),
        in_specs=[vmem] * 11 + [hbm] * 3,
        out_specs=(vmem, vmem),
        scratch_shapes=[
            pltpu.VMEM((NC, NY, NZ, 2 * length, width), BF16),
            pltpu.VMEM((n_tp, 3, part, model), BF16),
            pltpu.VMEM((n_ep, CAP, model), BF16),
            pltpu.VMEM((n_ep, CAP, model), BF16),
            pltpu.VMEM((slots, model), BF16),
            pltpu.VMEM((slots, model), F32),
            pltpu.VMEM((n_ep, CAP, model), BF16),
            pltpu.VMEM((n_ep, CAP, model), BF16),
            pltpu.VMEM((width, heads * length), BF16),
            pltpu.VMEM((width, heads * length), F32),
            pltpu.VMEM((8, heads * length), F32),
            pltpu.VMEM((slots, rows_here), BF16),
            pltpu.VMEM((2, rows_here, slots), BF16),
            dma((3,)),
            dma((2, 3, 3)),
            dma((2, 3, 3)),
            dma((NZ,)),
            dma((NZ,)),
            dma((2, 3)),
            dma((2, 3)),
            dma((NY,)),
            dma((NY,)),
            dma((n_ep,)),
            dma((n_ep,)),
            dma((n_ep,)),
            dma((n_ep,)),
        ],
        compiler_params=pltpu.CompilerParams(
            collective_id=0, has_side_effects=True, vmem_limit_bytes=60 * 1024 * 1024
        ),
    )(
        queries.reshape(length, heads * width), keys.reshape(length, width), values.reshape(length, width),
        query_gain.reshape(1, width), key_gain.reshape(1, width), cosine, sine,
        routed_rows, mixture_gain.reshape(1, model), expert_index, route_weights,
        expert_gate, expert_up, expert_down,
    )
    return attended.reshape(length, heads, width), combined


def solution(mesh):
    assert dict(mesh.shape) == {"ep": NZ * NY * NC, "tp": 4}
    placed = (
        P("ep", "tp", None),
        P("ep", "tp", None),
        P("ep", "tp", None),
        P(),
        P(),
        P(("ep", "tp"), None),
        P(),
        P(("ep", "tp"), None),
        P(("ep", "tp"), None),
        P("ep", "tp", None),
        P("ep", "tp", None),
        P("ep", "tp", None),
    )
    return jax.shard_map(
        on_device,
        mesh=mesh,
        in_specs=placed,
        out_specs=(P("ep", "tp", None), P(("ep", "tp"), None)),
        check_vma=False,
    )
```

```python
import functools

import jax
import jax.numpy as jnp
import numpy as np
from jax import lax
from jax.experimental import pallas as pl
from jax.experimental.pallas import tpu as pltpu
from jax.sharding import PartitionSpec as P

GROUPS = 4
GRID_W = 64
NZ, NY, NC = 8, 4, 2
CAP = 8
LOG2E = 1.4426950408889634

epsilon = 1e-06
rotary_base = 10000.0
floor_value = -1e30

F32 = jnp.float32
BF16 = jnp.bfloat16


def rms(values_f, gain):
    mean = jnp.mean(values_f * values_f, axis=-1, keepdims=True)
    return values_f * lax.rsqrt(mean + epsilon) * gain


def step_kernel(
    n_tp,
    q_hbm, k_hbm, v_hbm, rows_hbm, row_hbm, col_hbm, gate_ref, up_ref, down_ref,
    qg_ref, kg_ref, mg_ref, ei_ref, rw_ref,
    att_ref, comb_ref,
    q_ref, k_ref, v_ref, rows_ref, row_ref, col_ref,
    kv, wbuf, out, arr, arr16, total, res, ret, qt, acc, stat, dmat, place,
    in_sem, loc_sem, ws_sem, wr_sem, zs_sem, zr_sem, ys_sem, yr_sem, cs_sem, cr_sem,
    ds_sem, dr_sem, rs_sem, rr_sem, go_sem,
):
    me = lax.axis_index("ep")
    t = lax.axis_index("tp")
    z, y, c = me // (NY * NC), (me // NC) % NY, me % NC
    n_ep = NZ * NY * NC
    plane = NZ * NY

    def ep_of(zz, yy, cc):
        return zz * (NY * NC) + yy * NC + cc

    def ahead(k):
        dz, dy, dc = k % NZ, (k // NZ) % NY, k // plane
        return ep_of((z + dz) % NZ, (y + dy) % NY, (c + dc) % NC)

    def behind(k):
        dz, dy, dc = k % NZ, (k // NZ) % NY, k // plane
        return ep_of((z + NZ - dz) % NZ, (y + NY - dy) % NY, (c + NC - dc) % NC)

    def remote(src, dst, s_sem, r_sem, ep, tp):
        return pltpu.make_async_remote_copy(
            src_ref=src, dst_ref=dst, send_sem=s_sem, recv_sem=r_sem,
            device_id=(ep, tp), device_id_type=pl.DeviceIdType.MESH,
        )

    t_next, t_prev = (t + 1) % n_tp, (t + n_tp - 1) % n_tp
    partner = ep_of(z, y, (c + 1) % NC)

    barrier = pltpu.get_barrier_semaphore()
    for peer in (t_next, t_prev):
        pl.semaphore_signal(barrier, inc=1, device_id=(me, peer), device_id_type=pl.DeviceIdType.MESH)

    @pl.loop(1, n_ep)
    def _(k):
        pl.semaphore_signal(barrier, inc=1, device_id=(ahead(k), t), device_id_type=pl.DeviceIdType.MESH)

    half = wbuf.shape[2] // 2
    srcs = (gate_ref, up_ref, down_ref)
    reads = [
        pltpu.make_async_copy(src, dst, in_sem.at[i])
        for i, (src, dst) in enumerate(
            (
                (k_hbm, k_ref), (v_hbm, v_ref), (row_hbm.at[me], row_ref), (col_hbm, col_ref),
                (rows_hbm, rows_ref), (q_hbm, q_ref),
            )
        )
    ]
    for read in reads:
        read.start()

    def w_local(p):
        return pltpu.make_async_copy(srcs[p].at[0], wbuf.at[t, p], loc_sem.at[p])

    pl.semaphore_wait(barrier, n_ep - 1 + 2)

    def w_copy(d, stage, p):
        to = t_next if d == 0 else t_prev
        part = pl.ds(0, half) if (d == 0) != (stage == 1) else pl.ds(half, half)
        sems = (ws_sem.at[d, stage, p], wr_sem.at[d, stage, p])
        if stage < 2:
            return remote(srcs[p].at[0, part], wbuf.at[t, p, part], *sems, me, to)
        held = t_prev if d == 0 else t_next
        return remote(wbuf.at[held, p, part], wbuf.at[held, p, part], *sems, me, to)

    def each_w(stage, act):
        for p in range(3):
            for d in range(2):
                act(w_copy(d, stage, p))

    def start_weights():
        for stage in range(2):
            each_w(stage, lambda copy: copy.start())

    def forward_weights():
        for p in range(3):
            for d in range(2):
                w_copy(d, 0, p).wait_recv()
                w_copy(d, 2, p).start()

    @pl.when(c == 0)
    def _():
        start_weights()

    for p in range(3):
        w_local(p).start()

    for read in reads[:4]:
        read.wait()
    length, width = k_ref.shape
    lines = row_ref.shape[1]
    tables = [
        (row_ref[i][:, None, :] + col_ref[i][None, :, :]).reshape(length, width) for i in range(2)
    ]

    def turn(x, gain):
        n = rms(x.astype(F32), gain)
        return (n * tables[0] + pltpu.roll(n, width // 2, 1) * tables[1]).astype(BF16)

    kv[c, y, z, 0:length, :] = turn(k_ref[...], kg_ref[...])
    v_t = v_ref[...].astype(F32).T.astype(BF16)
    for j in range(length // width):
        kv[c, y, z, length + j * width : length + (j + 1) * width, :] = v_t[:, j * width : (j + 1) * width]

    def z_copy(j):
        step = {1: 1, 7: -1, 2: 2, 6: -2, 3: 1, 5: -1, 4: 2, 0: -2}[j]
        held = z if j in (1, 7, 2, 6) else (z + (NZ - 2 if j in (3, 4) else 2)) % NZ
        piece = kv.at[c, y, held]
        if j == 4:
            piece = kv.at[c, y, held, pl.ds(0, length)]
        if j == 0:
            piece = kv.at[c, y, held, pl.ds(length, length)]
        return remote(piece, piece, zs_sem.at[j], zr_sem.at[j], ep_of((z + step + NZ) % NZ, y, c), t)

    rows_here, model = rows_ref.shape
    pad = jnp.zeros((6, rows_here), F32)
    ids = jnp.concatenate([ei_ref[...].astype(F32), pad], axis=0).T
    lanes = lax.broadcasted_iota(jnp.int32, (rows_here, n_ep), 1).astype(F32)
    hot = [(ids[:, k : k + 1] == lanes).astype(F32) for k in range(2)]
    above = (
        lax.broadcasted_iota(jnp.int32, (rows_here, rows_here), 1)
        < lax.broadcasted_iota(jnp.int32, (rows_here, rows_here), 0)
    ).astype(F32).astype(BF16)
    earlier = jnp.dot(above, (hot[0] + hot[1]).astype(BF16), preferred_element_type=F32)
    slots = lax.broadcasted_iota(jnp.int32, (rows_here, n_ep * CAP), 1).astype(F32)
    picks = []
    for k in range(2):
        at = ids[:, k : k + 1] * CAP + jnp.sum(earlier * hot[k], axis=1, keepdims=True)
        pick = (at == slots).astype(F32)
        place[k] = pick.astype(BF16)
        picks.append(pick)
    dmat[...] = (picks[0] + picks[1]).T.astype(BF16)

    for j in (2, 6, 1, 7):
        z_copy(j).start()

    reads[4].wait()
    arr16[0:rows_here, :] = rms(rows_ref[...].astype(F32), mg_ref[...]).astype(BF16)

    @pl.loop(0, n_ep * CAP // 128)
    def _(i):
        block = jnp.dot(
            dmat[pl.ds(i * 128, 128), :], arr16[0:rows_here, :], preferred_element_type=F32
        )
        out[pl.ds(i * (128 // CAP), 128 // CAP)] = block.reshape(128 // CAP, CAP, model).astype(BF16)

    reads[5].wait()
    for h in range(q_ref.shape[1] // width):
        turned = turn(q_ref[:, h * width : (h + 1) * width], qg_ref[...])
        qt[:, h * length : (h + 1) * length] = turned.astype(F32).T.astype(BF16)

    def d_copy(k):
        return remote(out.at[ahead(k)], arr.at[k], ds_sem.at[k], dr_sem.at[k], ahead(k), t)

    def dispatch(core):
        @pl.loop(0, plane)
        def _(i):
            k = i + plane * ((c + core) % NC)

            @pl.when(k > 0)
            def _():
                d_copy(k).start()

    dispatch(0)
    own = pltpu.make_async_copy(out.at[me], arr.at[0], ds_sem.at[0])
    own.start()
    for j, after in ((2, (3, 4)), (6, (5, 0))):
        z_copy(j).wait_recv()
        for i in after:
            z_copy(i).start()
    dispatch(1)

    zh = NZ // 2

    def y_copy(d, stage):
        to = (y + 1) % NY if d == 0 else (y + NY - 1) % NY
        part = pl.ds(0, zh) if (d == 0) != (stage == 1) else pl.ds(zh, zh)
        held = y if stage < 2 else ((y + NY - 1) % NY if d == 0 else (y + 1) % NY)
        piece = kv.at[c, held, part]
        return remote(piece, piece, ys_sem.at[d, stage], yr_sem.at[d, stage], ep_of(z, to, c), t)

    def c_copy(dy):
        piece = kv.at[c, (y + dy) % NY]
        return remote(piece, piece, cs_sem.at[dy], cr_sem.at[dy], partner, t)

    def start_y():
        for j in (1, 7, 3, 5, 4, 0):
            z_copy(j).wait_recv()
        for stage in range(2):
            for d in range(2):
                y_copy(d, stage).start()
        c_copy(0).start()

    def forward_y():
        for d in range(2):
            y_copy(d, 0).wait_recv()
            y_copy(d, 2).start()

    def near_y():
        for d in range(2):
            y_copy(d, 1).wait_recv()
        c_copy(1).start()
        c_copy(3).start()

    def far_y():
        for d in range(2):
            y_copy(d, 2).wait_recv()
        c_copy(2).start()

    step = 256
    chunks = n_ep * CAP // step
    contract = (((1,), (1,)), ((), ()))

    def expert(q, i):
        at = pl.ds(i * step, step)
        x = arr16[at, :]
        g = lax.dot_general(x, wbuf[q, 0], contract, preferred_element_type=F32)
        u = lax.dot_general(x, wbuf[q, 1], contract, preferred_element_type=F32)
        hidden = (g / (1.0 + jnp.exp(-g)) * u).astype(BF16)
        part = jnp.dot(hidden, wbuf[q, 2], preferred_element_type=F32)
        return at, part.astype(BF16).astype(F32)

    def first_part():
        own.wait()
        for p in range(3):
            w_local(p).wait()
        group = 128 // CAP

        @pl.loop(0, n_ep // group)
        def _(i):
            @pl.loop(0, group)
            def _(j):
                k = i * group + j

                @pl.when(k > 0)
                def _():
                    d_copy(k).wait_recv()

            block = arr[pl.ds(i * group, group)].astype(F32)
            arr16[pl.ds(i * 128, 128), :] = block.reshape(128, model).astype(BF16)

        @pl.loop(0, chunks)
        def _(i):
            at, part = expert(t, i)
            total[at, :] = part

    def add_part(held):
        @pl.loop(0, chunks)
        def _(i):
            at, part = expert(held, i)
            total[at, :] = total[at, :] + part

    def r_copy(k):
        return remote(res.at[k], ret.at[me], rs_sem.at[k], rr_sem.at[k], behind(k), t)

    def r_wait(k):
        return remote(res.at[k], ret.at[ahead(k)], rs_sem.at[k], rr_sem.at[k], behind(k), t)

    mine = pltpu.make_async_copy(res.at[0], ret.at[me], rs_sem.at[0])

    def last_part():
        last = (t + 2) % n_tp
        per = step // CAP

        @pl.loop(0, chunks)
        def _(i):
            at, part = expert(last, i)
            block = (total[at, :] + part).astype(BF16).astype(F32)
            res[pl.ds(i * per, per)] = block.reshape(per, CAP, model).astype(BF16)

        @pl.loop(1, n_ep)
        def _(k):
            r_copy(k).start()

        mine.start()

    cols = qt.shape[1]
    factor = width ** (-0.5) * LOG2E
    stat[0:1, :] = jnp.full((1, cols), floor_value, F32)
    stat[1:2, :] = jnp.zeros((1, cols), F32)
    acc[...] = jnp.zeros_like(acc)

    def one_block(cc, yy, zz):
        k_block = kv[cc, yy, zz, 0:length, :]
        v_block = jnp.concatenate(
            [kv[cc, yy, zz, length + j * width : length + (j + 1) * width, :] for j in range(length // width)],
            axis=1,
        )
        s = jnp.dot(k_block, qt[...], preferred_element_type=F32)
        m_b = jnp.max(s, axis=0, keepdims=True)
        p = jnp.exp2((s - m_b) * factor)
        l_b = jnp.sum(p, axis=0, keepdims=True)
        a_b = jnp.dot(v_block, p.astype(BF16), preferred_element_type=F32)
        return m_b, l_b, a_b

    def attend(dy):
        c_copy(dy).wait_recv()
        yy = (y + dy) % NY

        @pl.loop(0, NZ * NC // 2)
        def _(b):
            cc, zz = b // zh, b % zh
            m_0, l_0, a_0 = one_block(cc, yy, 2 * zz)
            m_1, l_1, a_1 = one_block(cc, yy, 2 * zz + 1)
            m_old = stat[0:1, :]
            top = jnp.maximum(jnp.maximum(m_0, m_1), m_old)
            keep = jnp.exp2((m_old - top) * factor)
            n_0 = jnp.exp2((m_0 - top) * factor)
            n_1 = jnp.exp2((m_1 - top) * factor)
            stat[0:1, :] = top
            stat[1:2, :] = stat[1:2, :] * keep + l_0 * n_0 + l_1 * n_1
            acc[...] = acc[...] * keep + a_0 * n_0 + a_1 * n_1

    @pl.when(c == 0)
    def _():
        forward_weights()
        start_y()
        attend(0)
        first_part()
        each_w(1, lambda copy: copy.wait_recv())
        add_part(t_prev)
        each_w(2, lambda copy: copy.wait_send())
        pl.semaphore_signal(go_sem, inc=1, device_id=(partner, t), device_id_type=pl.DeviceIdType.MESH)
        add_part(t_next)
        each_w(2, lambda copy: copy.wait_recv())
        last_part()
        forward_y()
        near_y()
        attend(1)
        attend(3)

    @pl.when(c == 1)
    def _():
        start_y()
        attend(0)
        pl.semaphore_wait(go_sem, 1)
        start_weights()
        forward_y()
        forward_weights()
        first_part()
        each_w(1, lambda copy: copy.wait_recv())
        add_part(t_prev)
        add_part(t_next)
        near_y()
        attend(1)
        each_w(2, lambda copy: copy.wait_recv())
        last_part()
        attend(3)
        each_w(2, lambda copy: copy.wait_send())

    far_y()
    attend(2)
    done = acc[...] / stat[1:2, :]
    for h in range(cols // length):
        att_ref[:, h * width : (h + 1) * width] = done[:, h * length : (h + 1) * length].T.astype(BF16)

    weights = jnp.concatenate([rw_ref[...], pad], axis=0).T

    @pl.loop(1, n_ep)
    def _(k):
        r_wait(k).wait_recv()

    mine.wait()

    @pl.loop(0, n_ep * CAP // 128)
    def _(i):
        block = ret[pl.ds(i * (128 // CAP), 128 // CAP)].astype(F32)
        arr16[pl.ds(i * 128, 128), :] = block.reshape(128, model).astype(BF16)

    wide = 512
    for j in range(model // wide):
        block = arr16[:, j * wide : (j + 1) * wide]
        picked = [jnp.dot(place[k], block, preferred_element_type=F32) * weights[:, k : k + 1] for k in range(2)]
        comb_ref[:, j * wide : (j + 1) * wide] = (picked[0] + picked[1]).astype(BF16)

    for stage in range(2):
        each_w(stage, lambda copy: copy.wait_send())
    for stage in range(3):
        for d in range(2):
            y_copy(d, stage).wait_send()
    for j in range(NZ):
        z_copy(j).wait_send()
    for dy in range(NY):
        c_copy(dy).wait_send()

    @pl.loop(1, n_ep)
    def _(k):
        d_copy(k).wait_send()
        r_copy(k).wait_send()


def position_tables(count, width):
    quarter = width // 4
    frequency = np.float32(rotary_base) ** (-np.arange(quarter, dtype=np.float32) / np.float32(quarter))
    none = np.zeros((1, quarter))

    def laid(n, first):
        angle = (np.arange(n, dtype=np.float32)[:, None] * frequency).astype(np.float64)
        tables = []
        for value, sign in ((np.cos(angle), 1.0), (np.sin(angle), -1.0)):
            blank = np.broadcast_to(none, value.shape)
            pair = (value, blank) if first else (blank, value)
            tables.append(np.concatenate([sign * pair[0], sign * pair[1], *pair], axis=1))
        return np.stack(tables).astype(np.float32)

    rows = laid(count // GRID_W, True)
    return rows, laid(GRID_W, False)


def on_device(
    queries, keys, values, query_gain, key_gain, routed_rows, mixture_gain,
    expert_index, route_weights, expert_gate, expert_up, expert_down,
):
    length, heads, width = queries.shape
    rows_here, model = routed_rows.shape
    n_tp = lax.axis_size("tp")
    n_ep = lax.axis_size("ep")
    slots = n_ep * CAP
    part = expert_gate.shape[1]
    rows, columns = position_tables(n_ep * length, width)
    rows = jnp.asarray(np.moveaxis(rows.reshape(2, n_ep, length // GRID_W, width), 1, 0))
    vmem = pl.BlockSpec(memory_space=pltpu.VMEM)
    hbm = pl.BlockSpec(memory_space=pl.ANY)
    dma = pltpu.SemaphoreType.DMA
    attended, combined = pl.pallas_call(
        functools.partial(step_kernel, n_tp),
        name="step",
        out_shape=(
            jax.ShapeDtypeStruct((length, heads * width), BF16),
            jax.ShapeDtypeStruct((rows_here, model), BF16),
        ),
        in_specs=[hbm] * 9 + [vmem] * 5,
        out_specs=(vmem, vmem),
        scratch_shapes=[
            pltpu.VMEM((length, heads * width), BF16),
            pltpu.VMEM((length, width), BF16),
            pltpu.VMEM((length, width), BF16),
            pltpu.VMEM((rows_here, model), BF16),
            pltpu.VMEM((2, length // GRID_W, width), F32),
            pltpu.VMEM((2, GRID_W, width), F32),
            pltpu.VMEM((NC, NY, NZ, 2 * length, width), BF16),
            pltpu.VMEM((n_tp, 3, part, model), BF16),
            pltpu.VMEM((n_ep, CAP, model), BF16),
            pltpu.VMEM((n_ep, CAP, model), BF16),
            pltpu.VMEM((slots, model), BF16),
            pltpu.VMEM((slots, model), F32),
            pltpu.VMEM((n_ep, CAP, model), BF16),
            pltpu.VMEM((n_ep, CAP, model), BF16),
            pltpu.VMEM((width, heads * length), BF16),
            pltpu.VMEM((width, heads * length), F32),
            pltpu.VMEM((8, heads * length), F32),
            pltpu.VMEM((slots, rows_here), BF16),
            pltpu.VMEM((2, rows_here, slots), BF16),
            dma((6,)),
            dma((3,)),
            dma((2, 3, 3)),
            dma((2, 3, 3)),
            dma((NZ,)),
            dma((NZ,)),
            dma((2, 3)),
            dma((2, 3)),
            dma((NY,)),
            dma((NY,)),
            dma((n_ep,)),
            dma((n_ep,)),
            dma((n_ep,)),
            dma((n_ep,)),
            pltpu.SemaphoreType.REGULAR,
        ],
        compiler_params=pltpu.CompilerParams(
            collective_id=0, has_side_effects=True, vmem_limit_bytes=60 * 1024 * 1024
        ),
    )(
        queries.reshape(length, heads * width), keys.reshape(length, width), values.reshape(length, width),
        routed_rows, rows, jnp.asarray(columns), expert_gate, expert_up, expert_down,
        query_gain.reshape(1, width), key_gain.reshape(1, width), mixture_gain.reshape(1, model),
        expert_index.T, route_weights.T,
    )
    return attended.reshape(length, heads, width), combined


def solution(mesh):
    assert dict(mesh.shape) == {"ep": NZ * NY * NC, "tp": 4}
    placed = (
        P("ep", "tp", None),
        P("ep", "tp", None),
        P("ep", "tp", None),
        P(),
        P(),
        P(("ep", "tp"), None),
        P(),
        P(("ep", "tp"), None),
        P(("ep", "tp"), None),
        P("ep", "tp", None),
        P("ep", "tp", None),
        P("ep", "tp", None),
    )
    return jax.shard_map(
        on_device,
        mesh=mesh,
        in_specs=placed,
        out_specs=(P("ep", "tp", None), P(("ep", "tp"), None)),
        check_vma=False,
    )
```

```python
import functools

import jax
import jax.numpy as jnp
import numpy as np
from jax import lax
from jax.experimental import pallas as pl
from jax.experimental.pallas import tpu as pltpu
from jax.sharding import PartitionSpec as P

GROUPS = 4
GRID_W = 64
NZ, NY, NC = 8, 4, 2
CAP = 8
LOG2E = 1.4426950408889634

epsilon = 1e-06
rotary_base = 10000.0
floor_value = -1e30

F32 = jnp.float32
BF16 = jnp.bfloat16


def rms(values_f, gain):
    mean = jnp.mean(values_f * values_f, axis=-1, keepdims=True)
    return values_f * lax.rsqrt(mean + epsilon) * gain


def step_kernel(
    n_tp,
    q_hbm, k_hbm, v_hbm, rows_hbm, row_hbm, col_hbm, gate_ref, up_ref, down_ref,
    qg_ref, kg_ref, mg_ref, ei_ref, rw_ref,
    att_ref, comb_ref,
    q_ref, k_ref, v_ref, rows_ref, row_ref, col_ref,
    kv, wbuf, out, arr, arr16, total, res, ret, qt, acc, stat, dmat, place,
    in_sem, loc_sem, ws_sem, wr_sem, zs_sem, zr_sem, ys_sem, yr_sem, cs_sem, cr_sem,
    ds_sem, dr_sem, rs_sem, rr_sem, go_sem,
):
    me = lax.axis_index("ep")
    t = lax.axis_index("tp")
    z, y, c = me // (NY * NC), (me // NC) % NY, me % NC
    n_ep = NZ * NY * NC
    plane = NZ * NY

    def ep_of(zz, yy, cc):
        return zz * (NY * NC) + yy * NC + cc

    def ahead(k):
        dz, dy, dc = k % NZ, (k // NZ) % NY, k // plane
        return ep_of((z + dz) % NZ, (y + dy) % NY, (c + dc) % NC)

    def behind(k):
        dz, dy, dc = k % NZ, (k // NZ) % NY, k // plane
        return ep_of((z + NZ - dz) % NZ, (y + NY - dy) % NY, (c + NC - dc) % NC)

    def remote(src, dst, s_sem, r_sem, ep, tp):
        return pltpu.make_async_remote_copy(
            src_ref=src, dst_ref=dst, send_sem=s_sem, recv_sem=r_sem,
            device_id=(ep, tp), device_id_type=pl.DeviceIdType.MESH,
        )

    t_next, t_prev = (t + 1) % n_tp, (t + n_tp - 1) % n_tp
    partner = ep_of(z, y, (c + 1) % NC)

    barrier = pltpu.get_barrier_semaphore()
    for peer in (t_next, t_prev):
        pl.semaphore_signal(barrier, inc=1, device_id=(me, peer), device_id_type=pl.DeviceIdType.MESH)

    z_at = [(z + dz) % NZ for dz in range(NZ)]
    y_at = [(y + dy) % NY for dy in range(NY)]
    for dy in (2, 1, 3, 0):
        for dz in (4, 3, 5, 2, 6, 1, 7, 0):
            for dc in range(NC):
                if dz + dy + dc > 0:
                    peer = ep_of(z_at[dz], y_at[dy], (c + dc) % NC)
                    pl.semaphore_signal(barrier, inc=1, device_id=(peer, t), device_id_type=pl.DeviceIdType.MESH)

    half = wbuf.shape[2] // 2
    srcs = (gate_ref, up_ref, down_ref)
    reads = [
        pltpu.make_async_copy(src, dst, in_sem.at[i])
        for i, (src, dst) in enumerate(
            (
                (k_hbm, k_ref), (v_hbm, v_ref), (row_hbm.at[me], row_ref), (col_hbm, col_ref),
                (rows_hbm, rows_ref), (q_hbm, q_ref),
            )
        )
    ]
    for read in reads:
        read.start()

    def w_local(p):
        return pltpu.make_async_copy(srcs[p].at[0], wbuf.at[t, p], loc_sem.at[p])

    pl.semaphore_wait(barrier, n_ep - 1 + 2)

    def w_copy(d, stage, p):
        to = t_next if d == 0 else t_prev
        part = pl.ds(0, half) if (d == 0) != (stage == 1) else pl.ds(half, half)
        sems = (ws_sem.at[d, stage, p], wr_sem.at[d, stage, p])
        if stage < 2:
            return remote(srcs[p].at[0, part], wbuf.at[t, p, part], *sems, me, to)
        held = t_prev if d == 0 else t_next
        return remote(wbuf.at[held, p, part], wbuf.at[held, p, part], *sems, me, to)

    def each_w(stage, act):
        for p in range(3):
            for d in range(2):
                act(w_copy(d, stage, p))

    def start_weights():
        for stage in range(2):
            each_w(stage, lambda copy: copy.start())

    def forward_weights():
        for p in range(3):
            for d in range(2):
                w_copy(d, 0, p).wait_recv()
                w_copy(d, 2, p).start()

    @pl.when(c == 0)
    def _():
        start_weights()

    for p in range(3):
        w_local(p).start()

    for read in reads[:4]:
        read.wait()
    length, width = k_ref.shape
    lines = row_ref.shape[1]
    tables = [
        (row_ref[i][:, None, :] + col_ref[i][None, :, :]).reshape(length, width) for i in range(2)
    ]

    def turn(x, gain):
        n = rms(x.astype(F32), gain)
        return (n * tables[0] + pltpu.roll(n, width // 2, 1) * tables[1]).astype(BF16)

    kv[c, y, z, 0:length, :] = turn(k_ref[...], kg_ref[...])
    v_t = v_ref[...].astype(F32).T.astype(BF16)
    for j in range(length // width):
        kv[c, y, z, length + j * width : length + (j + 1) * width, :] = v_t[:, j * width : (j + 1) * width]

    def z_copy(j):
        step = {1: 1, 7: -1, 2: 2, 6: -2, 3: 1, 5: -1, 4: 2, 0: -2}[j]
        held = z if j in (1, 7, 2, 6) else (z + (NZ - 2 if j in (3, 4) else 2)) % NZ
        piece = kv.at[c, y, held]
        if j == 4:
            piece = kv.at[c, y, held, pl.ds(0, length)]
        if j == 0:
            piece = kv.at[c, y, held, pl.ds(length, length)]
        return remote(piece, piece, zs_sem.at[j], zr_sem.at[j], ep_of((z + step + NZ) % NZ, y, c), t)

    rows_here, model = rows_ref.shape
    pad = jnp.zeros((6, rows_here), F32)
    ids = jnp.concatenate([ei_ref[...].astype(F32), pad], axis=0).T
    lanes = lax.broadcasted_iota(jnp.int32, (rows_here, n_ep), 1).astype(F32)
    hot = [(ids[:, k : k + 1] == lanes).astype(F32) for k in range(2)]
    above = (
        lax.broadcasted_iota(jnp.int32, (rows_here, rows_here), 1)
        < lax.broadcasted_iota(jnp.int32, (rows_here, rows_here), 0)
    ).astype(F32).astype(BF16)
    earlier = jnp.dot(above, (hot[0] + hot[1]).astype(BF16), preferred_element_type=F32)
    slots = lax.broadcasted_iota(jnp.int32, (rows_here, n_ep * CAP), 1).astype(F32)
    picks = []
    for k in range(2):
        at = ids[:, k : k + 1] * CAP + jnp.sum(earlier * hot[k], axis=1, keepdims=True)
        pick = (at == slots).astype(F32)
        place[k] = pick.astype(BF16)
        picks.append(pick)
    dmat[...] = (picks[0] + picks[1]).T.astype(BF16)

    for j in (2, 6, 1, 7):
        z_copy(j).start()

    reads[4].wait()
    arr16[0:rows_here, :] = rms(rows_ref[...].astype(F32), mg_ref[...]).astype(BF16)

    @pl.loop(0, n_ep * CAP // 128)
    def _(i):
        block = jnp.dot(
            dmat[pl.ds(i * 128, 128), :], arr16[0:rows_here, :], preferred_element_type=F32
        )
        out[pl.ds(i * (128 // CAP), 128 // CAP)] = block.reshape(128 // CAP, CAP, model).astype(BF16)

    def d_copy(k):
        return remote(out.at[ahead(k)], arr.at[k], ds_sem.at[k], dr_sem.at[k], ahead(k), t)

    def dispatch(core):
        @pl.loop(0, plane)
        def _(i):
            k = i + plane * ((c + core) % NC)

            @pl.when(k > 0)
            def _():
                d_copy(k).start()

    own = pltpu.make_async_copy(out.at[me], arr.at[0], ds_sem.at[0])
    own.start()
    for j, after in ((2, (3, 4)), (6, (5, 0))):
        z_copy(j).wait_recv()
        for i in after:
            z_copy(i).start()
    dispatch(0)
    dispatch(1)

    reads[5].wait()
    for h in range(q_ref.shape[1] // width):
        turned = turn(q_ref[:, h * width : (h + 1) * width], qg_ref[...])
        qt[:, h * length : (h + 1) * length] = turned.astype(F32).T.astype(BF16)

    zh = NZ // 2

    def y_copy(d, stage):
        to = (y + 1) % NY if d == 0 else (y + NY - 1) % NY
        part = pl.ds(0, zh) if (d == 0) != (stage == 1) else pl.ds(zh, zh)
        held = y if stage < 2 else ((y + NY - 1) % NY if d == 0 else (y + 1) % NY)
        piece = kv.at[c, held, part]
        return remote(piece, piece, ys_sem.at[d, stage], yr_sem.at[d, stage], ep_of(z, to, c), t)

    def c_copy(dy):
        piece = kv.at[c, (y + dy) % NY]
        return remote(piece, piece, cs_sem.at[dy], cr_sem.at[dy], partner, t)

    def start_y():
        for j in (1, 7, 3, 5, 4, 0):
            z_copy(j).wait_recv()
        for stage in range(2):
            for d in range(2):
                y_copy(d, stage).start()
        c_copy(0).start()

    def forward_y():
        for d in range(2):
            y_copy(d, 0).wait_recv()
            y_copy(d, 2).start()

    def near_y():
        for d in range(2):
            y_copy(d, 1).wait_recv()
        c_copy(1).start()
        c_copy(3).start()

    def far_y():
        for d in range(2):
            y_copy(d, 2).wait_recv()
        c_copy(2).start()

    step = 256
    chunks = n_ep * CAP // step
    contract = (((1,), (1,)), ((), ()))

    def expert(q, i):
        at = pl.ds(i * step, step)
        x = arr16[at, :]
        g = lax.dot_general(x, wbuf[q, 0], contract, preferred_element_type=F32)
        u = lax.dot_general(x, wbuf[q, 1], contract, preferred_element_type=F32)
        hidden = (g / (1.0 + jnp.exp(-g)) * u).astype(BF16)
        part = jnp.dot(hidden, wbuf[q, 2], preferred_element_type=F32)
        return at, part.astype(BF16).astype(F32)

    def first_part():
        own.wait()
        for p in range(3):
            w_local(p).wait()
        group = 128 // CAP

        @pl.loop(0, n_ep // group)
        def _(i):
            @pl.loop(0, group)
            def _(j):
                k = i * group + j

                @pl.when(k > 0)
                def _():
                    d_copy(k).wait_recv()

            block = arr[pl.ds(i * group, group)].astype(F32)
            arr16[pl.ds(i * 128, 128), :] = block.reshape(128, model).astype(BF16)

        @pl.loop(0, chunks)
        def _(i):
            at, part = expert(t, i)
            total[at, :] = part

    def add_part(held):
        @pl.loop(0, chunks)
        def _(i):
            at, part = expert(held, i)
            total[at, :] = total[at, :] + part

    def r_copy(k):
        return remote(res.at[k], ret.at[me], rs_sem.at[k], rr_sem.at[k], behind(k), t)

    def r_wait(k):
        return remote(res.at[k], ret.at[ahead(k)], rs_sem.at[k], rr_sem.at[k], behind(k), t)

    mine = pltpu.make_async_copy(res.at[0], ret.at[me], rs_sem.at[0])

    def last_part():
        last = (t + 2) % n_tp
        per = step // CAP

        @pl.loop(0, chunks)
        def _(i):
            at, part = expert(last, i)
            block = (total[at, :] + part).astype(BF16).astype(F32)
            res[pl.ds(i * per, per)] = block.reshape(per, CAP, model).astype(BF16)

            @pl.loop(0, per)
            def _(j):
                k = i * per + j

                @pl.when(k > 0)
                def _():
                    r_copy(k).start()

        mine.start()

    cols = qt.shape[1]
    factor = width ** (-0.5) * LOG2E
    stat[0:1, :] = jnp.full((1, cols), floor_value, F32)
    stat[1:2, :] = jnp.zeros((1, cols), F32)
    acc[...] = jnp.zeros_like(acc)

    def one_block(cc, yy, zz):
        k_block = kv[cc, yy, zz, 0:length, :]
        v_block = jnp.concatenate(
            [kv[cc, yy, zz, length + j * width : length + (j + 1) * width, :] for j in range(length // width)],
            axis=1,
        )
        s = jnp.dot(k_block, qt[...], preferred_element_type=F32)
        m_b = jnp.max(s, axis=0, keepdims=True)
        p = jnp.exp2((s - m_b) * factor)
        l_b = jnp.sum(p, axis=0, keepdims=True)
        a_b = jnp.dot(v_block, p.astype(BF16), preferred_element_type=F32)
        return m_b, l_b, a_b

    def attend(dy):
        c_copy(dy).wait_recv()
        yy = (y + dy) % NY

        @pl.loop(0, NZ * NC // 2)
        def _(b):
            cc, zz = b // zh, b % zh
            m_0, l_0, a_0 = one_block(cc, yy, 2 * zz)
            m_1, l_1, a_1 = one_block(cc, yy, 2 * zz + 1)
            m_old = stat[0:1, :]
            top = jnp.maximum(jnp.maximum(m_0, m_1), m_old)
            keep = jnp.exp2((m_old - top) * factor)
            n_0 = jnp.exp2((m_0 - top) * factor)
            n_1 = jnp.exp2((m_1 - top) * factor)
            stat[0:1, :] = top
            stat[1:2, :] = stat[1:2, :] * keep + l_0 * n_0 + l_1 * n_1
            acc[...] = acc[...] * keep + a_0 * n_0 + a_1 * n_1

    @pl.when(c == 0)
    def _():
        forward_weights()
        start_y()
        attend(0)
        each_w(2, lambda copy: copy.wait_send())
        pl.semaphore_signal(go_sem, inc=1, device_id=(partner, t), device_id_type=pl.DeviceIdType.MESH)
        forward_y()
        first_part()
        each_w(1, lambda copy: copy.wait_recv())
        add_part(t_prev)
        add_part(t_next)
        each_w(2, lambda copy: copy.wait_recv())
        last_part()
        near_y()
        attend(1)
        attend(3)
        far_y()
        attend(2)

    @pl.when(c == 1)
    def _():
        start_y()
        attend(0)
        forward_y()
        pl.semaphore_wait(go_sem, 1)
        start_weights()
        near_y()
        forward_weights()
        first_part()
        each_w(1, lambda copy: copy.wait_recv())
        add_part(t_prev)
        add_part(t_next)
        attend(1)
        far_y()
        each_w(2, lambda copy: copy.wait_recv())
        last_part()
        attend(3)
        attend(2)
        each_w(2, lambda copy: copy.wait_send())

    done = acc[...] / stat[1:2, :]
    for h in range(cols // length):
        att_ref[:, h * width : (h + 1) * width] = done[:, h * length : (h + 1) * length].T.astype(BF16)

    weights = jnp.concatenate([rw_ref[...], pad], axis=0).T

    @pl.loop(1, n_ep)
    def _(k):
        r_wait(k).wait_recv()

    mine.wait()

    @pl.loop(0, n_ep * CAP // 128)
    def _(i):
        block = ret[pl.ds(i * (128 // CAP), 128 // CAP)].astype(F32)
        arr16[pl.ds(i * 128, 128), :] = block.reshape(128, model).astype(BF16)

    wide = 512
    for j in range(model // wide):
        block = arr16[:, j * wide : (j + 1) * wide]
        picked = [jnp.dot(place[k], block, preferred_element_type=F32) * weights[:, k : k + 1] for k in range(2)]
        comb_ref[:, j * wide : (j + 1) * wide] = (picked[0] + picked[1]).astype(BF16)

    for stage in range(2):
        each_w(stage, lambda copy: copy.wait_send())
    for stage in range(3):
        for d in range(2):
            y_copy(d, stage).wait_send()
    for j in range(NZ):
        z_copy(j).wait_send()
    for dy in range(NY):
        c_copy(dy).wait_send()

    @pl.loop(1, n_ep)
    def _(k):
        d_copy(k).wait_send()
        r_copy(k).wait_send()


def position_tables(count, width):
    quarter = width // 4
    frequency = np.float32(rotary_base) ** (-np.arange(quarter, dtype=np.float32) / np.float32(quarter))
    none = np.zeros((1, quarter))

    def laid(n, first):
        angle = (np.arange(n, dtype=np.float32)[:, None] * frequency).astype(np.float64)
        tables = []
        for value, sign in ((np.cos(angle), 1.0), (np.sin(angle), -1.0)):
            blank = np.broadcast_to(none, value.shape)
            pair = (value, blank) if first else (blank, value)
            tables.append(np.concatenate([sign * pair[0], sign * pair[1], *pair], axis=1))
        return np.stack(tables).astype(np.float32)

    rows = laid(count // GRID_W, True)
    return rows, laid(GRID_W, False)


def on_device(
    queries, keys, values, query_gain, key_gain, routed_rows, mixture_gain,
    expert_index, route_weights, expert_gate, expert_up, expert_down,
):
    length, heads, width = queries.shape
    rows_here, model = routed_rows.shape
    n_tp = lax.axis_size("tp")
    n_ep = lax.axis_size("ep")
    slots = n_ep * CAP
    part = expert_gate.shape[1]
    rows, columns = position_tables(n_ep * length, width)
    rows = jnp.asarray(np.moveaxis(rows.reshape(2, n_ep, length // GRID_W, width), 1, 0))
    vmem = pl.BlockSpec(memory_space=pltpu.VMEM)
    hbm = pl.BlockSpec(memory_space=pl.ANY)
    dma = pltpu.SemaphoreType.DMA
    attended, combined = pl.pallas_call(
        functools.partial(step_kernel, n_tp),
        name="step",
        out_shape=(
            jax.ShapeDtypeStruct((length, heads * width), BF16),
            jax.ShapeDtypeStruct((rows_here, model), BF16),
        ),
        in_specs=[hbm] * 9 + [vmem] * 5,
        out_specs=(vmem, vmem),
        scratch_shapes=[
            pltpu.VMEM((length, heads * width), BF16),
            pltpu.VMEM((length, width), BF16),
            pltpu.VMEM((length, width), BF16),
            pltpu.VMEM((rows_here, model), BF16),
            pltpu.VMEM((2, length // GRID_W, width), F32),
            pltpu.VMEM((2, GRID_W, width), F32),
            pltpu.VMEM((NC, NY, NZ, 2 * length, width), BF16),
            pltpu.VMEM((n_tp, 3, part, model), BF16),
            pltpu.VMEM((n_ep, CAP, model), BF16),
            pltpu.VMEM((n_ep, CAP, model), BF16),
            pltpu.VMEM((slots, model), BF16),
            pltpu.VMEM((slots, model), F32),
            pltpu.VMEM((n_ep, CAP, model), BF16),
            pltpu.VMEM((n_ep, CAP, model), BF16),
            pltpu.VMEM((width, heads * length), BF16),
            pltpu.VMEM((width, heads * length), F32),
            pltpu.VMEM((8, heads * length), F32),
            pltpu.VMEM((slots, rows_here), BF16),
            pltpu.VMEM((2, rows_here, slots), BF16),
            dma((6,)),
            dma((3,)),
            dma((2, 3, 3)),
            dma((2, 3, 3)),
            dma((NZ,)),
            dma((NZ,)),
            dma((2, 3)),
            dma((2, 3)),
            dma((NY,)),
            dma((NY,)),
            dma((n_ep,)),
            dma((n_ep,)),
            dma((n_ep,)),
            dma((n_ep,)),
            pltpu.SemaphoreType.REGULAR,
        ],
        compiler_params=pltpu.CompilerParams(
            collective_id=0, has_side_effects=True, vmem_limit_bytes=60 * 1024 * 1024
        ),
    )(
        queries.reshape(length, heads * width), keys.reshape(length, width), values.reshape(length, width),
        routed_rows, rows, jnp.asarray(columns), expert_gate, expert_up, expert_down,
        query_gain.reshape(1, width), key_gain.reshape(1, width), mixture_gain.reshape(1, model),
        expert_index.T, route_weights.T,
    )
    return attended.reshape(length, heads, width), combined


def solution(mesh):
    assert dict(mesh.shape) == {"ep": NZ * NY * NC, "tp": 4}
    placed = (
        P("ep", "tp", None),
        P("ep", "tp", None),
        P("ep", "tp", None),
        P(),
        P(),
        P(("ep", "tp"), None),
        P(),
        P(("ep", "tp"), None),
        P(("ep", "tp"), None),
        P("ep", "tp", None),
        P("ep", "tp", None),
        P("ep", "tp", None),
    )
    return jax.shard_map(
        on_device,
        mesh=mesh,
        in_specs=placed,
        out_specs=(P("ep", "tp", None), P(("ep", "tp"), None)),
        check_vma=False,
    )
```

```python
import functools

import jax
import jax.numpy as jnp
import numpy as np
from jax import lax
from jax.experimental import pallas as pl
from jax.experimental.pallas import tpu as pltpu
from jax.sharding import PartitionSpec as P

GROUPS = 4
GRID_W = 64
NZ, NY, NC = 8, 4, 2
CAP = 8
LOG2E = 1.4426950408889634

epsilon = 1e-06
rotary_base = 10000.0
floor_value = -1e30

F32 = jnp.float32
BF16 = jnp.bfloat16


def rms(values_f, gain):
    mean = jnp.mean(values_f * values_f, axis=-1, keepdims=True)
    return values_f * lax.rsqrt(mean + epsilon) * gain


def step_kernel(
    n_tp,
    q_hbm, k_hbm, v_hbm, rows_hbm, row_hbm, col_hbm, gate_ref, up_ref, down_ref,
    qg_ref, kg_ref, mg_ref, ei_ref, rw_ref,
    att_out, comb_out,
    att_ref, comb_ref, q_ref, k_ref, v_ref, rows_ref, row_ref, col_ref,
    kv, wbuf, out, arr, arr16, total, hid, res, ret, qt, acc, stat, dmat, place,
    in_sem, out_sem, loc_sem, own_sem, ws_sem, wr_sem, zs_sem, zr_sem, ys_sem, yr_sem, cs_sem, cr_sem,
    ds_sem, dr_sem, rs_sem, rr_sem, go_sem,
):
    me = lax.axis_index("ep")
    t = lax.axis_index("tp")
    z, y, c = me // (NY * NC), (me // NC) % NY, me % NC
    n_ep = NZ * NY * NC
    plane = NZ * NY

    def ep_of(zz, yy, cc):
        return zz * (NY * NC) + yy * NC + cc

    def line(ep):
        return (ep % NC) * plane + ep // NC

    def remote(src, dst, s_sem, r_sem, ep, tp):
        return pltpu.make_async_remote_copy(
            src_ref=src, dst_ref=dst, send_sem=s_sem, recv_sem=r_sem,
            device_id=(ep, tp), device_id_type=pl.DeviceIdType.MESH,
        )

    def sent(ref, sem):
        remote(ref, ref, sem, sem, partner, t).wait_send()

    def landed(ref, sem):
        remote(ref, ref, sem, sem, partner, t).wait_recv()

    partner = ep_of(z, y, (c + 1) % NC)
    t_next, t_prev = (t + 1) % n_tp, (t + n_tp - 1) % n_tp

    barrier = pltpu.get_barrier_semaphore()
    for peer in (t_next, t_prev):
        pl.semaphore_signal(barrier, inc=1, device_id=(me, peer), device_id_type=pl.DeviceIdType.MESH)

    z_at = [(z + dz) % NZ for dz in range(NZ)]
    y_at = [(y + dy) % NY for dy in range(NY)]
    for dy in (2, 1, 3, 0):
        for dz in (4, 3, 5, 2, 6, 1, 7, 0):
            for dc in range(NC):
                if dz + dy + dc > 0:
                    peer = ep_of(z_at[dz], y_at[dy], (c + dc) % NC)
                    pl.semaphore_signal(barrier, inc=1, device_id=(peer, t), device_id_type=pl.DeviceIdType.MESH)

    half = wbuf.shape[2] // 2
    srcs = (gate_ref, up_ref, down_ref)
    reads = [
        pltpu.make_async_copy(src, dst, in_sem.at[i])
        for i, (src, dst) in enumerate(
            (
                (k_hbm, k_ref), (v_hbm, v_ref), (row_hbm.at[me], row_ref), (col_hbm, col_ref),
                (rows_hbm, rows_ref), (q_hbm, q_ref),
            )
        )
    ]
    for read in reads:
        read.start()

    def w_local(p):
        return pltpu.make_async_copy(srcs[p].at[0], wbuf.at[t, p], loc_sem.at[p])

    pl.semaphore_wait(barrier, n_ep - 1 + 2)

    def w_copy(d, stage, p):
        to = t_next if d == 0 else t_prev
        part = pl.ds(0, half) if (d == 0) != (stage == 1) else pl.ds(half, half)
        sems = (
            ws_sem.at[p if stage == 2 else 3],
            wr_sem.at[(3 * d + p, 6, 7 + p // 2)[stage]],
        )
        if stage < 2:
            return remote(srcs[p].at[0, part], wbuf.at[t, p, part], *sems, me, to)
        held = t_prev if d == 0 else t_next
        return remote(wbuf.at[held, p, part], wbuf.at[held, p, part], *sems, me, to)

    def each_w(stage, act):
        for p in range(3):
            for d in range(2):
                act(w_copy(d, stage, p))

    def start_weights():
        for stage in range(2):
            each_w(stage, lambda copy: copy.start())

    def forward_weights():
        for p in range(3):
            for d in range(2):
                w_copy(d, 0, p).wait_recv()
                w_copy(d, 2, p).start()

    @pl.when(c == 0)
    def _():
        start_weights()

    for p in range(3):
        w_local(p).start()

    for read in reads[:4]:
        read.wait()
    length, width = k_ref.shape
    lines = row_ref.shape[1]
    tables = [
        (row_ref[i][:, None, :] + col_ref[i][None, :, :]).reshape(length, width) for i in range(2)
    ]

    def turn(x, gain):
        n = rms(x.astype(F32), gain)
        return (n * tables[0] + pltpu.roll(n, width // 2, 1) * tables[1]).astype(BF16)

    kv[c, y, z, 0:length, :] = turn(k_ref[...], kg_ref[...])
    v_t = v_ref[...].astype(F32).T.astype(BF16)
    for j in range(length // width):
        kv[c, y, z, length + j * width : length + (j + 1) * width, :] = v_t[:, j * width : (j + 1) * width]

    def z_copy(j):
        step, back = {1: (1, 0), 2: (2, 0), 3: (1, 2), 4: (2, 2), 7: (-1, 0), 6: (-2, 0), 5: (-1, -2), 0: (-2, -2)}[j]
        held = (z - back + NZ) % NZ
        piece = kv.at[c, y, held]
        if j == 4:
            piece = kv.at[c, y, held, pl.ds(0, length)]
        if j == 0:
            piece = kv.at[c, y, held, pl.ds(length, length)]
        return remote(piece, piece, zs_sem.at[0], zr_sem.at[{2: 1, 6: 2}.get(j, 0)], ep_of((z + step + NZ) % NZ, y, c), t)

    rows_here, model = rows_ref.shape
    pad = jnp.zeros((6, rows_here), F32)
    ids = jnp.concatenate([ei_ref[...].astype(F32), pad], axis=0).T
    lanes = lax.broadcasted_iota(jnp.int32, (rows_here, n_ep), 1).astype(F32)
    hot = [(ids[:, k : k + 1] == lanes).astype(F32) for k in range(2)]
    above = (
        lax.broadcasted_iota(jnp.int32, (rows_here, rows_here), 1)
        < lax.broadcasted_iota(jnp.int32, (rows_here, rows_here), 0)
    ).astype(F32).astype(BF16)
    earlier = jnp.dot(above, (hot[0] + hot[1]).astype(BF16), preferred_element_type=F32)
    slots = lax.broadcasted_iota(jnp.int32, (rows_here, n_ep * CAP), 1).astype(F32)
    picks = []
    for k in range(2):
        upper = jnp.floor(ids[:, k : k + 1] * (1.0 / NC))
        row = (ids[:, k : k + 1] - upper * NC) * plane + upper
        at = row * CAP + jnp.sum(earlier * hot[k], axis=1, keepdims=True)
        pick = (at == slots).astype(F32)
        place[k] = pick.astype(BF16)
        picks.append(pick)
    dmat[...] = (picks[0] + picks[1]).T.astype(BF16)

    for j in (2, 6, 1, 7):
        z_copy(j).start()

    reads[4].wait()
    arr16[0:rows_here, :] = rms(rows_ref[...].astype(F32), mg_ref[...]).astype(BF16)

    @pl.loop(0, n_ep * CAP // 128)
    def _(i):
        block = jnp.dot(
            dmat[pl.ds(i * 128, 128), :], arr16[0:rows_here, :], preferred_element_type=F32
        )
        out[pl.ds(i * (128 // CAP), 128 // CAP)] = block.reshape(128 // CAP, CAP, model).astype(BF16)

    def alternate(i):
        side = 1 - 2 * (i % 2)
        return (NZ // 2 + side * ((i + 1) // 2) + NZ) % NZ

    def dispatch(core):
        dc = (c + core) % NC
        for dy in range(NY):

            @pl.loop(0, NZ)
            def _(i):
                dz = alternate(i)
                row = (z + dz) % NZ * NY + y_at[dy]
                k = dc * plane + dy * NZ + dz
                copy = remote(
                    out.at[core * plane + row], arr.at[k], ds_sem.at[0], dr_sem.at[2 * dc + dy // 2], row * NC + core, t
                )
                if dy > 0:
                    copy.start()
                else:
                    pl.when(k > 0)(copy.start)

    own = pltpu.make_async_copy(out.at[line(me)], arr.at[0], own_sem.at[0])
    own.start()
    for j, after in ((2, (3, 4)), (6, (5, 0))):
        z_copy(j).wait_recv()
        for i in after:
            z_copy(i).start()
    dispatch(0)
    dispatch(1)

    reads[5].wait()
    q_f = q_ref[...].astype(F32)
    for h in range(q_ref.shape[1]):
        turned = turn(q_f[:, h, :], qg_ref[...])
        qt[:, h * length : (h + 1) * length] = turned.astype(F32).T.astype(BF16)

    zh = NZ // 2

    def y_copy(d, stage):
        to = (y + 1) % NY if d == 0 else (y + NY - 1) % NY
        part = pl.ds(0, zh) if (d == 0) != (stage == 1) else pl.ds(zh, zh)
        held = y if stage < 2 else ((y + NY - 1) % NY if d == 0 else (y + 1) % NY)
        piece = kv.at[c, held, part]
        return remote(piece, piece, ys_sem.at[0], yr_sem.at[d if stage == 0 else stage + 1], ep_of(z, to, c), t)

    def c_copy(dy):
        piece = kv.at[c, (y + dy) % NY]
        return remote(piece, piece, cs_sem.at[0], cr_sem.at[dy], partner, t)

    def start_y():
        landed(kv.at[c, y, pl.ds(0, 5)], zr_sem.at[0])
        for stage in range(2):
            for d in range(2):
                y_copy(d, stage).start()
        c_copy(0).start()

    def forward_y():
        for d in range(2):
            y_copy(d, 0).wait_recv()
            y_copy(d, 2).start()

    def near_y():
        landed(kv.at[c, 0], yr_sem.at[2])
        c_copy(1).start()
        c_copy(3).start()

    def far_y():
        landed(kv.at[c, 0], yr_sem.at[3])
        c_copy(2).start()

    step = 256
    chunks = n_ep * CAP // step
    contract = (((1,), (1,)), ((), ()))

    def hidden_of(x, q):
        g = lax.dot_general(x, wbuf[q, 0], contract, preferred_element_type=F32)
        u = lax.dot_general(x, wbuf[q, 1], contract, preferred_element_type=F32)
        return (g / (1.0 + jnp.exp(-g)) * u).astype(BF16)

    def expert(q, i):
        at = pl.ds(i * step, step)
        part = jnp.dot(hidden_of(arr16[at, :], q), wbuf[q, 2], preferred_element_type=F32)
        return at, part.astype(BF16).astype(F32)

    def first_part():
        own.wait()
        for p in range(3):
            w_local(p).wait()
        group = 128 // CAP

        for i in range(n_ep // group):
            low = max(i * group, 1)
            landed(arr.at[pl.ds(low, (i + 1) * group - low)], dr_sem.at[i])
            block = arr[i * group : (i + 1) * group].astype(F32)
            arr16[i * 128 : (i + 1) * 128, :] = block.reshape(128, model).astype(BF16)

        @pl.loop(0, chunks)
        def _(i):
            at, part = expert(t, i)
            total[at, :] = part

    def add_part(held):
        @pl.loop(0, chunks)
        def _(i):
            at, part = expert(held, i)
            total[at, :] = total[at, :] + part

    mine = pltpu.make_async_copy(res.at[0], ret.at[line(me)], own_sem.at[1])

    def last_part():
        last = (t + 2) % n_tp
        per = step // CAP
        landed(wbuf.at[0, pl.ds(0, 2)], wr_sem.at[7])

        @pl.loop(0, chunks)
        def _(i):
            at = pl.ds(i * step, step)
            hid[at, :] = hidden_of(arr16[at, :], last)

        landed(wbuf.at[0, 2], wr_sem.at[8])

        @pl.loop(0, chunks)
        def _(i):
            at = pl.ds(i * step, step)
            part = jnp.dot(hid[at, :], wbuf[last, 2], preferred_element_type=F32).astype(BF16).astype(F32)
            block = (total[at, :] + part).astype(BF16).astype(F32)
            res[pl.ds(i * per, per)] = block.reshape(per, CAP, model).astype(BF16)

            core = (c + i) % NC

            for dy in range(NY):

                @pl.loop(0, NZ)
                def _(j):
                    dz = alternate(j)
                    row = (z + NZ - dz) % NZ * NY + y_at[(NY - dy) % NY]
                    k = i * plane + dy * NZ + dz
                    copy = remote(
                        res.at[k], ret.at[line(me)], rs_sem.at[0], rr_sem.at[i], row * NC + core, t
                    )
                    if dy > 0:
                        copy.start()
                    else:
                        pl.when(k > 0)(copy.start)

        mine.start()

    cols = qt.shape[1]
    factor = width ** (-0.5) * LOG2E
    stat[0:1, :] = jnp.full((1, cols), floor_value, F32)
    stat[1:2, :] = jnp.zeros((1, cols), F32)
    acc[...] = jnp.zeros_like(acc)

    def one_block(cc, yy, zz):
        k_block = kv[cc, yy, zz, 0:length, :]
        v_block = jnp.concatenate(
            [kv[cc, yy, zz, length + j * width : length + (j + 1) * width, :] for j in range(length // width)],
            axis=1,
        )
        s = jnp.dot(k_block, qt[...], preferred_element_type=F32)
        m_b = jnp.max(s, axis=0, keepdims=True)
        p = jnp.exp2((s - m_b) * factor)
        l_b = jnp.sum(p, axis=0, keepdims=True)
        a_b = jnp.dot(v_block, p.astype(BF16), preferred_element_type=F32)
        return m_b, l_b, a_b

    def attend(dy, core):
        yy = (y + dy) % NY

        @pl.loop(0, zh)
        def _(zz):
            cc = (c + core) % NC
            m_0, l_0, a_0 = one_block(cc, yy, 2 * zz)
            m_1, l_1, a_1 = one_block(cc, yy, 2 * zz + 1)
            m_old = stat[0:1, :]
            top = jnp.maximum(jnp.maximum(m_0, m_1), m_old)
            keep = jnp.exp2((m_old - top) * factor)
            n_0 = jnp.exp2((m_0 - top) * factor)
            n_1 = jnp.exp2((m_1 - top) * factor)
            stat[0:1, :] = top
            stat[1:2, :] = stat[1:2, :] * keep + l_0 * n_0 + l_1 * n_1
            acc[...] = acc[...] * keep + a_0 * n_0 + a_1 * n_1

    @pl.when(c == 0)
    def _():
        forward_weights()
        start_y()
        attend(0, 0)
        c_copy(0).wait_recv()
        attend(0, 1)
        for p in range(2):
            sent(wbuf.at[0, p], ws_sem.at[p])
        pl.semaphore_signal(go_sem, inc=1, device_id=(partner, t), device_id_type=pl.DeviceIdType.MESH)
        forward_y()
        first_part()
        landed(wbuf.at[0], wr_sem.at[6])
        add_part(t_prev)
        add_part(t_next)
        last_part()
        near_y()
        for dy in (1, 3):
            attend(dy, 0)
        for dy in (1, 3):
            c_copy(dy).wait_recv()
            attend(dy, 1)
        far_y()
        attend(2, 0)
        c_copy(2).wait_recv()
        attend(2, 1)

    @pl.when(c == 1)
    def _():
        start_y()
        attend(0, 0)
        c_copy(0).wait_recv()
        attend(0, 1)
        forward_y()
        pl.semaphore_wait(go_sem, 1)
        start_weights()
        near_y()
        attend(1, 0)
        forward_weights()
        attend(3, 0)
        first_part()
        landed(wbuf.at[0], wr_sem.at[6])
        add_part(t_prev)
        add_part(t_next)
        far_y()
        attend(2, 0)
        last_part()
        for dy in (1, 3, 2):
            c_copy(dy).wait_recv()
            attend(dy, 1)
        for p in range(2):
            sent(wbuf.at[0, p], ws_sem.at[p])

    done = acc[...] / stat[1:2, :]
    heads = [done[:, h * length : (h + 1) * length].T for h in range(cols // length)]
    att_ref[...] = jnp.stack(heads, axis=1).astype(BF16)
    writes = [pltpu.make_async_copy(att_ref, att_out, out_sem.at[4])]
    writes[0].start()

    sent(wbuf.at[pl.ds(0, 2)], ws_sem.at[3])
    sent(wbuf.at[0, 2], ws_sem.at[2])
    sent(kv.at[c, y, pl.ds(0, NZ - 1)], zs_sem.at[0])
    sent(kv.at[c, pl.ds(0, NY - 1)], ys_sem.at[0])
    sent(kv.at[c], cs_sem.at[0])
    sent(out.at[pl.ds(0, n_ep - 1)], ds_sem.at[0])

    weights = jnp.concatenate([rw_ref[...], pad], axis=0).T
    wide = 512

    def take(core):
        @pl.when(c == core)
        def _():
            landed(ret.at[pl.ds(core * plane, plane - 1)], rr_sem.at[0])
            mine.wait()

        @pl.when(c != core)
        def _():
            landed(ret.at[pl.ds(core * plane, plane)], rr_sem.at[1])

        lines = plane * CAP
        for i in range(lines // 128):
            first = core * plane + i * (128 // CAP)
            block = ret[first : first + 128 // CAP].astype(F32)
            arr16[first * CAP : first * CAP + 128, :] = block.reshape(128, model).astype(BF16)
        for j in range(model // wide):
            block = arr16[core * lines : (core + 1) * lines, j * wide : (j + 1) * wide]
            picked = [
                jnp.dot(place[k, :, core * lines : (core + 1) * lines], block, preferred_element_type=F32)
                * weights[:, k : k + 1]
                for k in range(2)
            ]
            yield pl.ds(j * wide, wide), picked[0] + picked[1]

    for at, value in take(0):
        total[0:rows_here, at] = value

    sent(res.at[pl.ds(0, n_ep - 1)], rs_sem.at[0])

    for i, (at, value) in enumerate(take(1)):
        comb_ref[:, at] = (total[0:rows_here, at] + value).astype(BF16)
        writes.append(pltpu.make_async_copy(comb_ref.at[:, at], comb_out.at[:, at], out_sem.at[i]))
        writes[-1].start()
    for write in writes:
        write.wait()


def position_tables(count, width):
    quarter = width // 4
    frequency = np.float32(rotary_base) ** (-np.arange(quarter, dtype=np.float32) / np.float32(quarter))
    none = np.zeros((1, quarter))

    def laid(n, first):
        angle = (np.arange(n, dtype=np.float32)[:, None] * frequency).astype(np.float64)
        tables = []
        for value, sign in ((np.cos(angle), 1.0), (np.sin(angle), -1.0)):
            blank = np.broadcast_to(none, value.shape)
            pair = (value, blank) if first else (blank, value)
            tables.append(np.concatenate([sign * pair[0], sign * pair[1], *pair], axis=1))
        return np.stack(tables).astype(np.float32)

    rows = laid(count // GRID_W, True)
    return rows, laid(GRID_W, False)


def on_device(
    queries, keys, values, query_gain, key_gain, routed_rows, mixture_gain,
    expert_index, route_weights, expert_gate, expert_up, expert_down,
):
    length, heads, width = queries.shape
    rows_here, model = routed_rows.shape
    n_tp = lax.axis_size("tp")
    n_ep = lax.axis_size("ep")
    slots = n_ep * CAP
    part = expert_gate.shape[1]
    rows, columns = position_tables(n_ep * length, width)
    rows = jnp.asarray(np.moveaxis(rows.reshape(2, n_ep, length // GRID_W, width), 1, 0))
    vmem = pl.BlockSpec(memory_space=pltpu.VMEM)
    hbm = pl.BlockSpec(memory_space=pl.ANY)
    dma = pltpu.SemaphoreType.DMA
    attended, combined = pl.pallas_call(
        functools.partial(step_kernel, n_tp),
        name="step",
        out_shape=(
            jax.ShapeDtypeStruct((length, heads, width), BF16),
            jax.ShapeDtypeStruct((rows_here, model), BF16),
        ),
        in_specs=[hbm] * 9 + [vmem] * 5,
        out_specs=(hbm, hbm),
        scratch_shapes=[
            pltpu.VMEM((length, heads, width), BF16),
            pltpu.VMEM((rows_here, model), BF16),
            pltpu.VMEM((length, heads, width), BF16),
            pltpu.VMEM((length, width), BF16),
            pltpu.VMEM((length, width), BF16),
            pltpu.VMEM((rows_here, model), BF16),
            pltpu.VMEM((2, length // GRID_W, width), F32),
            pltpu.VMEM((2, GRID_W, width), F32),
            pltpu.VMEM((NC, NY, NZ, 2 * length, width), BF16),
            pltpu.VMEM((n_tp, 3, part, model), BF16),
            pltpu.VMEM((n_ep, CAP, model), BF16),
            pltpu.VMEM((n_ep, CAP, model), BF16),
            pltpu.VMEM((slots, model), BF16),
            pltpu.VMEM((slots, model), F32),
            pltpu.VMEM((slots, part), BF16),
            pltpu.VMEM((n_ep, CAP, model), BF16),
            pltpu.VMEM((n_ep, CAP, model), BF16),
            pltpu.VMEM((width, heads * length), BF16),
            pltpu.VMEM((width, heads * length), F32),
            pltpu.VMEM((8, heads * length), F32),
            pltpu.VMEM((slots, rows_here), BF16),
            pltpu.VMEM((2, rows_here, slots), BF16),
            dma((6,)),
            dma((5,)),
            dma((3,)),
            dma((2,)),
            dma((4,)),
            dma((9,)),
            dma((1,)),
            dma((3,)),
            dma((1,)),
            dma((4,)),
            dma((1,)),
            dma((NY,)),
            dma((1,)),
            dma((4,)),
            dma((1,)),
            dma((2,)),
            pltpu.SemaphoreType.REGULAR,
        ],
        compiler_params=pltpu.CompilerParams(
            collective_id=0, has_side_effects=True, vmem_limit_bytes=60 * 1024 * 1024
        ),
    )(
        queries, keys.reshape(length, width), values.reshape(length, width),
        routed_rows, rows, jnp.asarray(columns), expert_gate, expert_up, expert_down,
        query_gain.reshape(1, width), key_gain.reshape(1, width), mixture_gain.reshape(1, model),
        expert_index.T, route_weights.T,
    )
    return attended, combined


def solution(mesh):
    assert dict(mesh.shape) == {"ep": NZ * NY * NC, "tp": 4}
    placed = (
        P("ep", "tp", None),
        P("ep", "tp", None),
        P("ep", "tp", None),
        P(),
        P(),
        P(("ep", "tp"), None),
        P(),
        P(("ep", "tp"), None),
        P(("ep", "tp"), None),
        P("ep", "tp", None),
        P("ep", "tp", None),
        P("ep", "tp", None),
    )
    return jax.shard_map(
        on_device,
        mesh=mesh,
        in_specs=placed,
        out_specs=(P("ep", "tp", None), P(("ep", "tp"), None)),
        check_vma=False,
    )
```

```python
import functools

import jax
import jax.numpy as jnp
import numpy as np
from jax import lax
from jax.experimental import pallas as pl
from jax.experimental.pallas import tpu as pltpu
from jax.sharding import PartitionSpec as P

GROUPS = 4
GRID_W = 64
NZ, NY, NC = 8, 4, 2
CAP = 8
LOG2E = 1.4426950408889634

epsilon = 1e-06
rotary_base = 10000.0
floor_value = -1e30

F32 = jnp.float32
BF16 = jnp.bfloat16


def rms(values_f, gain):
    mean = jnp.mean(values_f * values_f, axis=-1, keepdims=True)
    return values_f * lax.rsqrt(mean + epsilon) * gain


def step_kernel(
    n_tp,
    q_hbm, k_hbm, v_hbm, rows_hbm, row_hbm, col_hbm, gate_ref, up_ref, down_ref,
    qg_ref, kg_ref, mg_ref, ei_ref, rw_ref,
    att_out, comb_out,
    att_ref, comb_ref, q_ref, k_ref, v_ref, rows_ref, row_ref, col_ref,
    kv, wbuf, out, arr, arr16, total, hid, res, ret, qt, acc, stat, dmat, place,
    in_sem, out_sem, loc_sem, own_sem, ws_sem, wr_sem, zs_sem, zr_sem, ys_sem, yr_sem, cs_sem, cr_sem,
    ds_sem, dr_sem, rs_sem, rr_sem, go_sem,
):
    me = lax.axis_index("ep")
    t = lax.axis_index("tp")
    z, y, c = me // (NY * NC), (me // NC) % NY, me % NC
    n_ep = NZ * NY * NC
    plane = NZ * NY

    def ep_of(zz, yy, cc):
        return zz * (NY * NC) + yy * NC + cc

    def line(ep):
        return (ep % NC) * plane + ep // NC

    def remote(src, dst, s_sem, r_sem, ep, tp):
        return pltpu.make_async_remote_copy(
            src_ref=src, dst_ref=dst, send_sem=s_sem, recv_sem=r_sem,
            device_id=(ep, tp), device_id_type=pl.DeviceIdType.MESH,
        )

    def sent(ref, sem):
        remote(ref, ref, sem, sem, partner, t).wait_send()

    def landed(ref, sem):
        remote(ref, ref, sem, sem, partner, t).wait_recv()

    partner = ep_of(z, y, (c + 1) % NC)
    t_next, t_prev = (t + 1) % n_tp, (t + n_tp - 1) % n_tp

    barrier = pltpu.get_barrier_semaphore()
    for peer in (t_next, t_prev):
        pl.semaphore_signal(barrier, inc=1, device_id=(me, peer), device_id_type=pl.DeviceIdType.MESH)

    z_at = [(z + dz) % NZ for dz in range(NZ)]
    y_at = [(y + dy) % NY for dy in range(NY)]
    for dy in (2, 1, 3, 0):
        for dz in (4, 3, 5, 2, 6, 1, 7, 0):
            for dc in range(NC):
                if dz + dy + dc > 0:
                    peer = ep_of(z_at[dz], y_at[dy], (c + dc) % NC)
                    pl.semaphore_signal(barrier, inc=1, device_id=(peer, t), device_id_type=pl.DeviceIdType.MESH)

    half = wbuf.shape[2] // 2
    srcs = (gate_ref, up_ref, down_ref)
    reads = [
        pltpu.make_async_copy(src, dst, in_sem.at[i])
        for i, (src, dst) in enumerate(
            (
                (k_hbm, k_ref), (v_hbm, v_ref), (row_hbm.at[me], row_ref), (col_hbm, col_ref),
                (rows_hbm, rows_ref), (q_hbm, q_ref),
            )
        )
    ]
    for read in reads:
        read.start()

    def w_local(p):
        return pltpu.make_async_copy(srcs[p].at[0], wbuf.at[t, p], loc_sem.at[p])

    pl.semaphore_wait(barrier, n_ep - 1 + 2)

    def w_copy(d, stage, p):
        to = t_next if d == 0 else t_prev
        part = pl.ds(0, half) if (d == 0) != (stage == 1) else pl.ds(half, half)
        sems = (
            ws_sem.at[p if stage == 2 else 3],
            wr_sem.at[(3 * d + p, 6, 7 + p // 2)[stage]],
        )
        if stage < 2:
            return remote(srcs[p].at[0, part], wbuf.at[t, p, part], *sems, me, to)
        held = t_prev if d == 0 else t_next
        return remote(wbuf.at[held, p, part], wbuf.at[held, p, part], *sems, me, to)

    def each_w(stage, act):
        for p in range(3):
            for d in range(2):
                act(w_copy(d, stage, p))

    def start_weights():
        for stage in range(2):
            each_w(stage, lambda copy: copy.start())

    def forward_weights():
        for p in range(3):
            for d in range(2):
                w_copy(d, 0, p).wait_recv()
                w_copy(d, 2, p).start()

    @pl.when(c == 0)
    def _():
        start_weights()

    for p in range(3):
        w_local(p).start()

    for read in reads[:4]:
        read.wait()
    length, width = k_ref.shape
    lines = row_ref.shape[1]
    tables = [
        (row_ref[i][:, None, :] + col_ref[i][None, :, :]).reshape(length, width) for i in range(2)
    ]

    def turn(x, gain):
        n = rms(x.astype(F32), gain)
        return (n * tables[0] + pltpu.roll(n, width // 2, 1) * tables[1]).astype(BF16)

    kv[c, y, z, 0:length, :] = turn(k_ref[...], kg_ref[...])
    v_t = v_ref[...].astype(F32).T.astype(BF16)
    for j in range(length // width):
        kv[c, y, z, length + j * width : length + (j + 1) * width, :] = v_t[:, j * width : (j + 1) * width]

    def z_copy(j):
        step, back = {1: (1, 0), 2: (1, 1), 3: (1, 2), 4: (1, 3), 7: (-1, 0), 6: (-1, -1), 5: (-1, -2), 0: (-1, -3)}[j]
        held = (z - back + NZ) % NZ
        piece = kv.at[c, y, held]
        if j == 4:
            piece = kv.at[c, y, held, pl.ds(0, length)]
        if j == 0:
            piece = kv.at[c, y, held, pl.ds(length, length)]
        return remote(piece, piece, zs_sem.at[0], zr_sem.at[{1: 1, 7: 2, 2: 3, 6: 4, 3: 5, 5: 6}.get(j, 0)], ep_of((z + step + NZ) % NZ, y, c), t)

    rows_here, model = rows_ref.shape
    pad = jnp.zeros((6, rows_here), F32)
    ids = jnp.concatenate([ei_ref[...].astype(F32), pad], axis=0).T
    lanes = lax.broadcasted_iota(jnp.int32, (rows_here, n_ep), 1).astype(F32)
    hot = [(ids[:, k : k + 1] == lanes).astype(F32) for k in range(2)]
    above = (
        lax.broadcasted_iota(jnp.int32, (rows_here, rows_here), 1)
        < lax.broadcasted_iota(jnp.int32, (rows_here, rows_here), 0)
    ).astype(F32).astype(BF16)
    earlier = jnp.dot(above, (hot[0] + hot[1]).astype(BF16), preferred_element_type=F32)
    slots = lax.broadcasted_iota(jnp.int32, (rows_here, n_ep * CAP), 1).astype(F32)
    picks = []
    for k in range(2):
        upper = jnp.floor(ids[:, k : k + 1] * (1.0 / NC))
        row = (ids[:, k : k + 1] - upper * NC) * plane + upper
        at = row * CAP + jnp.sum(earlier * hot[k], axis=1, keepdims=True)
        pick = (at == slots).astype(F32)
        place[k] = pick.astype(BF16)
        picks.append(pick)
    dmat[...] = (picks[0] + picks[1]).T.astype(BF16)

    for j in (1, 7):
        z_copy(j).start()

    reads[4].wait()
    arr16[0:rows_here, :] = rms(rows_ref[...].astype(F32), mg_ref[...]).astype(BF16)

    @pl.loop(0, n_ep * CAP // 128)
    def _(i):
        block = jnp.dot(
            dmat[pl.ds(i * 128, 128), :], arr16[0:rows_here, :], preferred_element_type=F32
        )
        out[pl.ds(i * (128 // CAP), 128 // CAP)] = block.reshape(128 // CAP, CAP, model).astype(BF16)

    def alternate(i):
        side = 1 - 2 * (i % 2)
        return (NZ // 2 + side * ((i + 1) // 2) + NZ) % NZ

    def beyond(i):
        return alternate(i) * (1 - i // 5)

    def send_row(core, dz, dy):
        dc = (c + core) % NC
        row = (z + dz) % NZ * NY + y_at[dy]
        k = dc * plane + dy * NZ + dz
        copy = remote(
            out.at[core * plane + row], arr.at[k], ds_sem.at[0], dr_sem.at[2 * dc + dy // 2], row * NC + core, t
        )
        if dy > 0:
            copy.start()
        else:
            pl.when(k > 0)(copy.start)

    own = pltpu.make_async_copy(out.at[line(me)], arr.at[0], own_sem.at[0])
    own.start()
    fill = [(core, dy) for core in range(NC) for dy in range(NY)]
    hops = ((1, 7), (2, 6), (3, 5), (4, 0))
    for i in range(4):
        if i > 0:
            for d in range(2):
                z_copy(hops[i - 1][d]).wait_recv()
                z_copy(hops[i][d]).start()
        for core, dy in fill[3 * i : 3 * (i + 1)] if i < 3 else fill[3 * 3 :]:
            send_row(core, 1, dy)
            send_row(core, NZ - 1, dy)

    def dispatch(core):
        for dy in range(NY):

            @pl.loop(0, NZ - 2)
            def _(i):
                dz = beyond(i)
                send_row(core, dz, dy)

    dispatch(0)
    dispatch(1)

    reads[5].wait()
    q_f = q_ref[...].astype(F32)
    for h in range(q_ref.shape[1]):
        turned = turn(q_f[:, h, :], qg_ref[...])
        qt[:, h * length : (h + 1) * length] = turned.astype(F32).T.astype(BF16)

    zh = NZ // 2

    def y_copy(d, stage):
        to = (y + 1) % NY if d == 0 else (y + NY - 1) % NY
        part = pl.ds(0, zh) if (d == 0) != (stage == 1) else pl.ds(zh, zh)
        held = y if stage < 2 else ((y + NY - 1) % NY if d == 0 else (y + 1) % NY)
        piece = kv.at[c, held, part]
        return remote(piece, piece, ys_sem.at[0], yr_sem.at[d if stage == 0 else stage + 1], ep_of(z, to, c), t)

    def c_copy(dy):
        piece = kv.at[c, (y + dy) % NY]
        return remote(piece, piece, cs_sem.at[0], cr_sem.at[dy], partner, t)

    def start_y():
        landed(kv.at[c, y, 0], zr_sem.at[0])
        for stage in range(2):
            for d in range(2):
                y_copy(d, stage).start()
        c_copy(0).start()

    def forward_y():
        for d in range(2):
            y_copy(d, 0).wait_recv()
            y_copy(d, 2).start()

    def near_y():
        landed(kv.at[c, 0], yr_sem.at[2])
        c_copy(1).start()
        c_copy(3).start()

    def far_y():
        landed(kv.at[c, 0], yr_sem.at[3])
        c_copy(2).start()

    step = 256
    chunks = n_ep * CAP // step
    contract = (((1,), (1,)), ((), ()))

    def hidden_of(x, q):
        g = lax.dot_general(x, wbuf[q, 0], contract, preferred_element_type=F32)
        u = lax.dot_general(x, wbuf[q, 1], contract, preferred_element_type=F32)
        return (g / (1.0 + jnp.exp(-g)) * u).astype(BF16)

    def expert(q, i):
        at = pl.ds(i * step, step)
        part = jnp.dot(hidden_of(arr16[at, :], q), wbuf[q, 2], preferred_element_type=F32)
        return at, part.astype(BF16).astype(F32)

    def first_part():
        own.wait()
        for p in range(3):
            w_local(p).wait()
        group = 128 // CAP

        for i in range(n_ep // group):
            low = max(i * group, 1)
            landed(arr.at[pl.ds(low, (i + 1) * group - low)], dr_sem.at[i])
            block = arr[i * group : (i + 1) * group].astype(F32)
            arr16[i * 128 : (i + 1) * 128, :] = block.reshape(128, model).astype(BF16)

        @pl.loop(0, chunks)
        def _(i):
            at, part = expert(t, i)
            total[at, :] = part

    def add_part(held):
        @pl.loop(0, chunks)
        def _(i):
            at, part = expert(held, i)
            total[at, :] = total[at, :] + part

    mine = pltpu.make_async_copy(res.at[0], ret.at[line(me)], own_sem.at[1])

    def last_part():
        last = (t + 2) % n_tp
        per = step // CAP
        landed(wbuf.at[0, pl.ds(0, 2)], wr_sem.at[7])

        @pl.loop(0, chunks)
        def _(i):
            at = pl.ds(i * step, step)
            hid[at, :] = hidden_of(arr16[at, :], last)

        landed(wbuf.at[0, 2], wr_sem.at[8])

        @pl.loop(0, chunks)
        def _(i):
            at = pl.ds(i * step, step)
            part = jnp.dot(hid[at, :], wbuf[last, 2], preferred_element_type=F32).astype(BF16).astype(F32)
            block = (total[at, :] + part).astype(BF16).astype(F32)
            res[pl.ds(i * per, per)] = block.reshape(per, CAP, model).astype(BF16)

            core = (c + i) % NC

            for dy in range(NY):

                @pl.loop(0, NZ)
                def _(j):
                    dz = alternate(j)
                    row = (z + NZ - dz) % NZ * NY + y_at[(NY - dy) % NY]
                    k = i * plane + dy * NZ + dz
                    copy = remote(
                        res.at[k], ret.at[line(me)], rs_sem.at[0], rr_sem.at[i], row * NC + core, t
                    )
                    if dy > 0:
                        copy.start()
                    else:
                        pl.when(k > 0)(copy.start)

        mine.start()

    cols = qt.shape[1]
    factor = width ** (-0.5) * LOG2E
    stat[0:1, :] = jnp.full((1, cols), floor_value, F32)
    stat[1:2, :] = jnp.zeros((1, cols), F32)
    acc[...] = jnp.zeros_like(acc)

    def one_block(cc, yy, zz):
        k_block = kv[cc, yy, zz, 0:length, :]
        v_block = jnp.concatenate(
            [kv[cc, yy, zz, length + j * width : length + (j + 1) * width, :] for j in range(length // width)],
            axis=1,
        )
        s = jnp.dot(k_block, qt[...], preferred_element_type=F32)
        m_b = jnp.max(s, axis=0, keepdims=True)
        p = jnp.exp2((s - m_b) * factor)
        l_b = jnp.sum(p, axis=0, keepdims=True)
        a_b = jnp.dot(v_block, p.astype(BF16), preferred_element_type=F32)
        return m_b, l_b, a_b

    def attend(dy, core):
        yy = (y + dy) % NY

        @pl.loop(0, zh)
        def _(zz):
            cc = (c + core) % NC
            m_0, l_0, a_0 = one_block(cc, yy, 2 * zz)
            m_1, l_1, a_1 = one_block(cc, yy, 2 * zz + 1)
            m_old = stat[0:1, :]
            top = jnp.maximum(jnp.maximum(m_0, m_1), m_old)
            keep = jnp.exp2((m_old - top) * factor)
            n_0 = jnp.exp2((m_0 - top) * factor)
            n_1 = jnp.exp2((m_1 - top) * factor)
            stat[0:1, :] = top
            stat[1:2, :] = stat[1:2, :] * keep + l_0 * n_0 + l_1 * n_1
            acc[...] = acc[...] * keep + a_0 * n_0 + a_1 * n_1

    @pl.when(c == 0)
    def _():
        forward_weights()
        start_y()
        attend(0, 0)
        c_copy(0).wait_recv()
        attend(0, 1)
        for p in range(2):
            sent(wbuf.at[0, p], ws_sem.at[p])
        pl.semaphore_signal(go_sem, inc=1, device_id=(partner, t), device_id_type=pl.DeviceIdType.MESH)
        forward_y()
        first_part()
        landed(wbuf.at[0], wr_sem.at[6])
        add_part(t_prev)
        add_part(t_next)
        last_part()
        near_y()
        for dy in (1, 3):
            attend(dy, 0)
        for dy in (1, 3):
            c_copy(dy).wait_recv()
            attend(dy, 1)
        far_y()
        attend(2, 0)
        c_copy(2).wait_recv()
        attend(2, 1)

    @pl.when(c == 1)
    def _():
        start_y()
        attend(0, 0)
        c_copy(0).wait_recv()
        attend(0, 1)
        forward_y()
        pl.semaphore_wait(go_sem, 1)
        start_weights()
        near_y()
        attend(1, 0)
        forward_weights()
        attend(3, 0)
        first_part()
        landed(wbuf.at[0], wr_sem.at[6])
        add_part(t_prev)
        add_part(t_next)
        far_y()
        attend(2, 0)
        last_part()
        for dy in (1, 3, 2):
            c_copy(dy).wait_recv()
            attend(dy, 1)
        for p in range(2):
            sent(wbuf.at[0, p], ws_sem.at[p])

    done = acc[...] / stat[1:2, :]
    heads = [done[:, h * length : (h + 1) * length].T for h in range(cols // length)]
    att_ref[...] = jnp.stack(heads, axis=1).astype(BF16)
    writes = [pltpu.make_async_copy(att_ref, att_out, out_sem.at[4])]
    writes[0].start()

    sent(wbuf.at[pl.ds(0, 2)], ws_sem.at[3])
    sent(wbuf.at[0, 2], ws_sem.at[2])
    sent(kv.at[c, y, pl.ds(0, NZ - 1)], zs_sem.at[0])
    sent(kv.at[c, pl.ds(0, NY - 1)], ys_sem.at[0])
    sent(kv.at[c], cs_sem.at[0])
    sent(out.at[pl.ds(0, n_ep - 1)], ds_sem.at[0])

    weights = jnp.concatenate([rw_ref[...], pad], axis=0).T
    wide = 512

    def take(core):
        @pl.when(c == core)
        def _():
            landed(ret.at[pl.ds(core * plane, plane - 1)], rr_sem.at[0])
            mine.wait()

        @pl.when(c != core)
        def _():
            landed(ret.at[pl.ds(core * plane, plane)], rr_sem.at[1])

        lines = plane * CAP
        for i in range(lines // 128):
            first = core * plane + i * (128 // CAP)
            block = ret[first : first + 128 // CAP].astype(F32)
            arr16[first * CAP : first * CAP + 128, :] = block.reshape(128, model).astype(BF16)
        for j in range(model // wide):
            block = arr16[core * lines : (core + 1) * lines, j * wide : (j + 1) * wide]
            picked = [
                jnp.dot(place[k, :, core * lines : (core + 1) * lines], block, preferred_element_type=F32)
                * weights[:, k : k + 1]
                for k in range(2)
            ]
            yield pl.ds(j * wide, wide), picked[0] + picked[1]

    for at, value in take(0):
        total[0:rows_here, at] = value

    sent(res.at[pl.ds(0, n_ep - 1)], rs_sem.at[0])

    for i, (at, value) in enumerate(take(1)):
        comb_ref[:, at] = (total[0:rows_here, at] + value).astype(BF16)
        writes.append(pltpu.make_async_copy(comb_ref.at[:, at], comb_out.at[:, at], out_sem.at[i]))
        writes[-1].start()
    for write in writes:
        write.wait()


def position_tables(count, width):
    quarter = width // 4
    frequency = np.float32(rotary_base) ** (-np.arange(quarter, dtype=np.float32) / np.float32(quarter))
    none = np.zeros((1, quarter))

    def laid(n, first):
        angle = (np.arange(n, dtype=np.float32)[:, None] * frequency).astype(np.float64)
        tables = []
        for value, sign in ((np.cos(angle), 1.0), (np.sin(angle), -1.0)):
            blank = np.broadcast_to(none, value.shape)
            pair = (value, blank) if first else (blank, value)
            tables.append(np.concatenate([sign * pair[0], sign * pair[1], *pair], axis=1))
        return np.stack(tables).astype(np.float32)

    rows = laid(count // GRID_W, True)
    return rows, laid(GRID_W, False)


def on_device(
    queries, keys, values, query_gain, key_gain, routed_rows, mixture_gain,
    expert_index, route_weights, expert_gate, expert_up, expert_down,
):
    length, heads, width = queries.shape
    rows_here, model = routed_rows.shape
    n_tp = lax.axis_size("tp")
    n_ep = lax.axis_size("ep")
    slots = n_ep * CAP
    part = expert_gate.shape[1]
    rows, columns = position_tables(n_ep * length, width)
    rows = jnp.asarray(np.moveaxis(rows.reshape(2, n_ep, length // GRID_W, width), 1, 0))
    vmem = pl.BlockSpec(memory_space=pltpu.VMEM)
    hbm = pl.BlockSpec(memory_space=pl.ANY)
    dma = pltpu.SemaphoreType.DMA
    attended, combined = pl.pallas_call(
        functools.partial(step_kernel, n_tp),
        name="step",
        out_shape=(
            jax.ShapeDtypeStruct((length, heads, width), BF16),
            jax.ShapeDtypeStruct((rows_here, model), BF16),
        ),
        in_specs=[hbm] * 9 + [vmem] * 5,
        out_specs=(hbm, hbm),
        scratch_shapes=[
            pltpu.VMEM((length, heads, width), BF16),
            pltpu.VMEM((rows_here, model), BF16),
            pltpu.VMEM((length, heads, width), BF16),
            pltpu.VMEM((length, width), BF16),
            pltpu.VMEM((length, width), BF16),
            pltpu.VMEM((rows_here, model), BF16),
            pltpu.VMEM((2, length // GRID_W, width), F32),
            pltpu.VMEM((2, GRID_W, width), F32),
            pltpu.VMEM((NC, NY, NZ, 2 * length, width), BF16),
            pltpu.VMEM((n_tp, 3, part, model), BF16),
            pltpu.VMEM((n_ep, CAP, model), BF16),
            pltpu.VMEM((n_ep, CAP, model), BF16),
            pltpu.VMEM((slots, model), BF16),
            pltpu.VMEM((slots, model), F32),
            pltpu.VMEM((slots, part), BF16),
            pltpu.VMEM((n_ep, CAP, model), BF16),
            pltpu.VMEM((n_ep, CAP, model), BF16),
            pltpu.VMEM((width, heads * length), BF16),
            pltpu.VMEM((width, heads * length), F32),
            pltpu.VMEM((8, heads * length), F32),
            pltpu.VMEM((slots, rows_here), BF16),
            pltpu.VMEM((2, rows_here, slots), BF16),
            dma((6,)),
            dma((5,)),
            dma((3,)),
            dma((2,)),
            dma((4,)),
            dma((9,)),
            dma((1,)),
            dma((7,)),
            dma((1,)),
            dma((4,)),
            dma((1,)),
            dma((NY,)),
            dma((1,)),
            dma((4,)),
            dma((1,)),
            dma((2,)),
            pltpu.SemaphoreType.REGULAR,
        ],
        compiler_params=pltpu.CompilerParams(
            collective_id=0, has_side_effects=True, vmem_limit_bytes=60 * 1024 * 1024
        ),
    )(
        queries, keys.reshape(length, width), values.reshape(length, width),
        routed_rows, rows, jnp.asarray(columns), expert_gate, expert_up, expert_down,
        query_gain.reshape(1, width), key_gain.reshape(1, width), mixture_gain.reshape(1, model),
        expert_index.T, route_weights.T,
    )
    return attended, combined


def solution(mesh):
    assert dict(mesh.shape) == {"ep": NZ * NY * NC, "tp": 4}
    placed = (
        P("ep", "tp", None),
        P("ep", "tp", None),
        P("ep", "tp", None),
        P(),
        P(),
        P(("ep", "tp"), None),
        P(),
        P(("ep", "tp"), None),
        P(("ep", "tp"), None),
        P("ep", "tp", None),
        P("ep", "tp", None),
        P("ep", "tp", None),
    )
    return jax.shard_map(
        on_device,
        mesh=mesh,
        in_specs=placed,
        out_specs=(P("ep", "tp", None), P(("ep", "tp"), None)),
        check_vma=False,
    )
```

```python
import functools

import jax
import jax.numpy as jnp
import numpy as np
from jax import lax
from jax.experimental import pallas as pl
from jax.experimental.pallas import tpu as pltpu
from jax.sharding import PartitionSpec as P

GROUPS = 4
GRID_W = 64
NZ, NY, NC = 8, 4, 2
CAP = 8
LOG2E = 1.4426950408889634

epsilon = 1e-06
rotary_base = 10000.0
floor_value = -1e30

F32 = jnp.float32
BF16 = jnp.bfloat16


def rms(values_f, gain):
    mean = jnp.mean(values_f * values_f, axis=-1, keepdims=True)
    return values_f * lax.rsqrt(mean + epsilon) * gain


def step_kernel(
    n_tp,
    q_hbm, k_hbm, v_hbm, rows_hbm, row_hbm, col_hbm, gate_ref, up_ref, down_ref,
    qg_hbm, kg_hbm, mg_hbm, ei_hbm, rw_hbm,
    att_ref, comb_ref,
    q_ref, k_ref, v_ref, rows_ref, row_ref, col_ref,
    qg_ref, kg_ref, mg_ref, ei_ref, rw_ref,
    kv, wbuf, out, arr, arr16, total, hid, res, ret, qt, acc, stat, dmat, place,
    in_sem, loc_sem, own_sem, ws_sem, wr_sem, zs_sem, zr_sem, ys_sem, yr_sem, cs_sem, cr_sem,
    ds_sem, dr_sem, rs_sem, rr_sem, go_sem,
):
    me = lax.axis_index("ep")
    t = lax.axis_index("tp")
    z, y, c = me // (NY * NC), (me // NC) % NY, me % NC
    n_ep = NZ * NY * NC
    plane = NZ * NY

    def ep_of(zz, yy, cc):
        return zz * (NY * NC) + yy * NC + cc

    def line(ep):
        return (ep % NC) * plane + ep // NC

    def remote(src, dst, s_sem, r_sem, ep, tp):
        return pltpu.make_async_remote_copy(
            src_ref=src, dst_ref=dst, send_sem=s_sem, recv_sem=r_sem,
            device_id=(ep, tp), device_id_type=pl.DeviceIdType.MESH,
        )

    def sent(ref, sem):
        remote(ref, ref, sem, sem, partner, t).wait_send()

    def landed(ref, sem):
        remote(ref, ref, sem, sem, partner, t).wait_recv()

    partner = ep_of(z, y, (c + 1) % NC)
    t_next, t_prev = (t + 1) % n_tp, (t + n_tp - 1) % n_tp

    barrier = pltpu.get_barrier_semaphore()
    for peer in (t_next, t_prev):
        pl.semaphore_signal(barrier, inc=1, device_id=(me, peer), device_id_type=pl.DeviceIdType.MESH)

    z_at = [(z + dz) % NZ for dz in range(NZ)]
    y_at = [(y + dy) % NY for dy in range(NY)]
    for dy in (2, 1, 3, 0):
        for dz in (4, 3, 5, 2, 6, 1, 7, 0):
            for dc in range(NC):
                if dz + dy + dc > 0:
                    peer = ep_of(z_at[dz], y_at[dy], (c + dc) % NC)
                    pl.semaphore_signal(barrier, inc=1, device_id=(peer, t), device_id_type=pl.DeviceIdType.MESH)

    half = wbuf.shape[2] // 2
    srcs = (gate_ref, up_ref, down_ref)
    reads = [
        pltpu.make_async_copy(src, dst, in_sem.at[i])
        for i, (src, dst) in enumerate(
            (
                (k_hbm, k_ref), (v_hbm, v_ref), (row_hbm.at[me], row_ref), (col_hbm, col_ref),
                (rows_hbm, rows_ref), (q_hbm, q_ref),
                (kg_hbm, kg_ref), (ei_hbm, ei_ref), (mg_hbm, mg_ref), (qg_hbm, qg_ref), (rw_hbm, rw_ref),
            )
        )
    ]
    for read in reads:
        read.start()

    def w_local(p):
        return pltpu.make_async_copy(srcs[p].at[0], wbuf.at[t, p], loc_sem.at[p])

    pl.semaphore_wait(barrier, n_ep - 1 + 2)

    def w_copy(d, stage, p):
        to = t_next if d == 0 else t_prev
        part = pl.ds(0, half) if (d == 0) != (stage == 1) else pl.ds(half, half)
        sems = (
            ws_sem.at[p if stage == 2 else 3],
            wr_sem.at[(3 * d + p, 6, 7 + p // 2)[stage]],
        )
        if stage < 2:
            return remote(srcs[p].at[0, part], wbuf.at[t, p, part], *sems, me, to)
        held = t_prev if d == 0 else t_next
        return remote(wbuf.at[held, p, part], wbuf.at[held, p, part], *sems, me, to)

    def each_w(stage, act):
        for p in range(3):
            for d in range(2):
                act(w_copy(d, stage, p))

    def start_weights():
        for stage in range(2):
            each_w(stage, lambda copy: copy.start())

    def forward_weights():
        for p in range(3):
            for d in range(2):
                w_copy(d, 0, p).wait_recv()
                w_copy(d, 2, p).start()

    @pl.when(c == 0)
    def _():
        start_weights()

    for p in range(3):
        w_local(p).start()

    for read in reads[:4] + reads[6:8]:
        read.wait()
    length, width = k_ref.shape
    lines = row_ref.shape[1]
    tables = [
        (row_ref[i][:, None, :] + col_ref[i][None, :, :]).reshape(length, width) for i in range(2)
    ]

    def turn(x, gain):
        n = rms(x.astype(F32), gain)
        return (n * tables[0] + pltpu.roll(n, width // 2, 1) * tables[1]).astype(BF16)

    kv[c, y, z, 0:length, :] = turn(k_ref[...], kg_ref[...])
    v_t = v_ref[...].astype(F32).T.astype(BF16)
    for j in range(length // width):
        kv[c, y, z, length + j * width : length + (j + 1) * width, :] = v_t[:, j * width : (j + 1) * width]

    def z_copy(j):
        step, back = {1: (1, 0), 2: (1, 1), 3: (1, 2), 4: (1, 3), 7: (-1, 0), 6: (-1, -1), 5: (-1, -2), 0: (-1, -3)}[j]
        held = (z - back + NZ) % NZ
        piece = kv.at[c, y, held]
        if j == 4:
            piece = kv.at[c, y, held, pl.ds(0, length)]
        if j == 0:
            piece = kv.at[c, y, held, pl.ds(length, length)]
        return remote(piece, piece, zs_sem.at[0], zr_sem.at[{1: 1, 7: 2, 2: 3, 6: 4, 3: 5, 5: 6}.get(j, 0)], ep_of((z + step + NZ) % NZ, y, c), t)

    rows_here, model = rows_ref.shape
    pad = jnp.zeros((6, rows_here), F32)
    ids = jnp.concatenate([ei_ref[...].astype(F32), pad], axis=0).T
    lanes = lax.broadcasted_iota(jnp.int32, (rows_here, n_ep), 1).astype(F32)
    hot = [(ids[:, k : k + 1] == lanes).astype(F32) for k in range(2)]
    above = (
        lax.broadcasted_iota(jnp.int32, (rows_here, rows_here), 1)
        < lax.broadcasted_iota(jnp.int32, (rows_here, rows_here), 0)
    ).astype(F32).astype(BF16)
    earlier = jnp.dot(above, (hot[0] + hot[1]).astype(BF16), preferred_element_type=F32)
    slots = lax.broadcasted_iota(jnp.int32, (rows_here, n_ep * CAP), 1).astype(F32)
    picks = []
    for k in range(2):
        upper = jnp.floor(ids[:, k : k + 1] * (1.0 / NC))
        row = (ids[:, k : k + 1] - upper * NC) * plane + upper
        at = row * CAP + jnp.sum(earlier * hot[k], axis=1, keepdims=True)
        pick = (at == slots).astype(F32)
        place[k] = pick.astype(BF16)
        picks.append(pick)
    dmat[...] = (picks[0] + picks[1]).T.astype(BF16)

    for j in (1, 7):
        z_copy(j).start()

    reads[4].wait()
    reads[8].wait()
    arr16[0:rows_here, :] = rms(rows_ref[...].astype(F32), mg_ref[...]).astype(BF16)

    @pl.loop(0, n_ep * CAP // 128)
    def _(i):
        block = jnp.dot(
            dmat[pl.ds(i * 128, 128), :], arr16[0:rows_here, :], preferred_element_type=F32
        )
        out[pl.ds(i * (128 // CAP), 128 // CAP)] = block.reshape(128 // CAP, CAP, model).astype(BF16)

    def alternate(i):
        side = 1 - 2 * (i % 2)
        return (NZ // 2 + side * ((i + 1) // 2) + NZ) % NZ

    def beyond(i):
        return alternate(i) * (1 - i // 5)

    def send_row(core, dz, dy):
        dc = (c + core) % NC
        row = (z + dz) % NZ * NY + y_at[dy]
        k = dc * plane + dy * NZ + dz
        copy = remote(
            out.at[core * plane + row], arr.at[k], ds_sem.at[0], dr_sem.at[2 * dc + dy // 2], row * NC + core, t
        )
        if dy > 0:
            copy.start()
        else:
            pl.when(k > 0)(copy.start)

    own = pltpu.make_async_copy(out.at[line(me)], arr.at[0], own_sem.at[0])
    own.start()
    fill = [(core, dy) for core in range(NC) for dy in range(NY)]
    hops = ((1, 7), (2, 6), (3, 5), (4, 0))
    for i in range(4):
        if i > 0:
            for d in range(2):
                z_copy(hops[i - 1][d]).wait_recv()
                z_copy(hops[i][d]).start()
        for core, dy in fill[3 * i : 3 * (i + 1)] if i < 3 else fill[3 * 3 :]:
            send_row(core, 1, dy)
            send_row(core, NZ - 1, dy)

    def dispatch(core):
        for dy in range(NY):

            @pl.loop(0, NZ - 2)
            def _(i):
                dz = beyond(i)
                send_row(core, dz, dy)

    dispatch(0)
    dispatch(1)

    reads[5].wait()
    reads[9].wait()
    q_f = q_ref[...].astype(F32)
    for h in range(q_ref.shape[1]):
        turned = turn(q_f[:, h, :], qg_ref[...])
        qt[:, h * length : (h + 1) * length] = turned.astype(F32).T.astype(BF16)

    zh = NZ // 2

    def y_copy(d, stage):
        to = (y + 1) % NY if d == 0 else (y + NY - 1) % NY
        part = pl.ds(0, zh) if (d == 0) != (stage == 1) else pl.ds(zh, zh)
        held = y if stage < 2 else ((y + NY - 1) % NY if d == 0 else (y + 1) % NY)
        piece = kv.at[c, held, part]
        return remote(piece, piece, ys_sem.at[0], yr_sem.at[d if stage == 0 else stage + 1], ep_of(z, to, c), t)

    def c_copy(dy):
        piece = kv.at[c, (y + dy) % NY]
        return remote(piece, piece, cs_sem.at[0], cr_sem.at[dy], partner, t)

    def start_y():
        landed(kv.at[c, y, 0], zr_sem.at[0])
        for stage in range(2):
            for d in range(2):
                y_copy(d, stage).start()
        c_copy(0).start()

    def forward_y():
        for d in range(2):
            y_copy(d, 0).wait_recv()
            y_copy(d, 2).start()

    def near_y():
        landed(kv.at[c, 0], yr_sem.at[2])
        c_copy(1).start()
        c_copy(3).start()

    def far_y():
        landed(kv.at[c, 0], yr_sem.at[3])
        c_copy(2).start()

    step = 256
    chunks = n_ep * CAP // step
    contract = (((1,), (1,)), ((), ()))

    def hidden_of(x, q):
        g = lax.dot_general(x, wbuf[q, 0], contract, preferred_element_type=F32)
        u = lax.dot_general(x, wbuf[q, 1], contract, preferred_element_type=F32)
        return (g / (1.0 + jnp.exp(-g)) * u).astype(BF16)

    def expert(q, i):
        at = pl.ds(i * step, step)
        part = jnp.dot(hidden_of(arr16[at, :], q), wbuf[q, 2], preferred_element_type=F32)
        return at, part.astype(BF16).astype(F32)

    def first_part():
        own.wait()
        for p in range(3):
            w_local(p).wait()
        group = 128 // CAP

        for i in range(n_ep // group):
            low = max(i * group, 1)
            landed(arr.at[pl.ds(low, (i + 1) * group - low)], dr_sem.at[i])
            block = arr[i * group : (i + 1) * group].astype(F32)
            arr16[i * 128 : (i + 1) * 128, :] = block.reshape(128, model).astype(BF16)

        @pl.loop(0, chunks)
        def _(i):
            at, part = expert(t, i)
            total[at, :] = part

    def add_part(held):
        @pl.loop(0, chunks)
        def _(i):
            at, part = expert(held, i)
            total[at, :] = total[at, :] + part

    mine = pltpu.make_async_copy(res.at[0], ret.at[line(me)], own_sem.at[1])

    def last_part():
        last = (t + 2) % n_tp
        per = step // CAP // 2
        landed(wbuf.at[0, pl.ds(0, 2)], wr_sem.at[7])

        @pl.loop(0, chunks)
        def _(i):
            at = pl.ds(i * step, step)
            hid[at, :] = hidden_of(arr16[at, :], last)

        landed(wbuf.at[0, 2], wr_sem.at[8])

        piece = step // 2

        @pl.loop(0, 2 * chunks)
        def _(i):
            at = pl.ds(i * piece, piece)
            part = jnp.dot(hid[at, :], wbuf[last, 2], preferred_element_type=F32).astype(BF16).astype(F32)
            block = (total[at, :] + part).astype(BF16).astype(F32)
            res[pl.ds(i * per, per)] = block.reshape(per, CAP, model).astype(BF16)

            dc = i // 2
            core = (c + dc) % NC

            for pair in range(2):
                dy = i % 2 * 2 + pair

                @pl.loop(0, NZ)
                def _(j):
                    dz = alternate(j)
                    row = (z + NZ - dz) % NZ * NY + (y + NY - dy) % NY
                    k = dc * plane + dy * NZ + dz
                    copy = remote(
                        res.at[k], ret.at[line(me)], rs_sem.at[0], rr_sem.at[dc], row * NC + core, t
                    )
                    pl.when(k > 0)(copy.start)

        mine.start()

    cols = qt.shape[1]
    factor = width ** (-0.5) * LOG2E
    stat[0:1, :] = jnp.full((1, cols), floor_value, F32)
    stat[1:2, :] = jnp.zeros((1, cols), F32)
    acc[...] = jnp.zeros_like(acc)

    def one_block(cc, yy, zz):
        k_block = kv[cc, yy, zz, 0:length, :]
        v_block = jnp.concatenate(
            [kv[cc, yy, zz, length + j * width : length + (j + 1) * width, :] for j in range(length // width)],
            axis=1,
        )
        s = jnp.dot(k_block, qt[...], preferred_element_type=F32)
        m_b = jnp.max(s, axis=0, keepdims=True)
        p = jnp.exp2((s - m_b) * factor)
        l_b = jnp.sum(p, axis=0, keepdims=True)
        a_b = jnp.dot(v_block, p.astype(BF16), preferred_element_type=F32)
        return m_b, l_b, a_b

    def attend(dy, core):
        yy = (y + dy) % NY

        @pl.loop(0, zh)
        def _(zz):
            cc = (c + core) % NC
            m_0, l_0, a_0 = one_block(cc, yy, 2 * zz)
            m_1, l_1, a_1 = one_block(cc, yy, 2 * zz + 1)
            m_old = stat[0:1, :]
            top = jnp.maximum(jnp.maximum(m_0, m_1), m_old)
            keep = jnp.exp2((m_old - top) * factor)
            n_0 = jnp.exp2((m_0 - top) * factor)
            n_1 = jnp.exp2((m_1 - top) * factor)
            stat[0:1, :] = top
            stat[1:2, :] = stat[1:2, :] * keep + l_0 * n_0 + l_1 * n_1
            acc[...] = acc[...] * keep + a_0 * n_0 + a_1 * n_1

    @pl.when(c == 0)
    def _():
        forward_weights()
        start_y()
        attend(0, 0)
        c_copy(0).wait_recv()
        attend(0, 1)
        for p in range(2):
            sent(wbuf.at[0, p], ws_sem.at[p])
        pl.semaphore_signal(go_sem, inc=1, device_id=(partner, t), device_id_type=pl.DeviceIdType.MESH)
        forward_y()
        first_part()
        landed(wbuf.at[0], wr_sem.at[6])
        add_part(t_prev)
        add_part(t_next)
        last_part()
        near_y()
        for dy in (1, 3):
            attend(dy, 0)
        for dy in (1, 3):
            c_copy(dy).wait_recv()
            attend(dy, 1)
        far_y()
        attend(2, 0)
        c_copy(2).wait_recv()
        attend(2, 1)

    @pl.when(c == 1)
    def _():
        start_y()
        attend(0, 0)
        c_copy(0).wait_recv()
        attend(0, 1)
        forward_y()
        pl.semaphore_wait(go_sem, 1)
        start_weights()
        near_y()
        attend(1, 0)
        forward_weights()
        attend(3, 0)
        first_part()
        landed(wbuf.at[0], wr_sem.at[6])
        add_part(t_prev)
        add_part(t_next)
        far_y()
        attend(2, 0)
        last_part()
        for dy in (1, 3, 2):
            c_copy(dy).wait_recv()
            attend(dy, 1)
        for p in range(2):
            sent(wbuf.at[0, p], ws_sem.at[p])

    done = acc[...] / stat[1:2, :]
    heads = [done[:, h * length : (h + 1) * length].T for h in range(cols // length)]
    att_ref[...] = jnp.stack(heads, axis=1).astype(BF16)

    sent(wbuf.at[pl.ds(0, 2)], ws_sem.at[3])
    sent(wbuf.at[0, 2], ws_sem.at[2])
    sent(kv.at[c, y, pl.ds(0, NZ - 1)], zs_sem.at[0])
    sent(kv.at[c, pl.ds(0, NY - 1)], ys_sem.at[0])
    sent(kv.at[c], cs_sem.at[0])
    sent(out.at[pl.ds(0, n_ep - 1)], ds_sem.at[0])

    reads[10].wait()
    weights = jnp.concatenate([rw_ref[...], pad], axis=0).T
    wide = 512

    def take(core):
        @pl.when(c == core)
        def _():
            landed(ret.at[pl.ds(core * plane, plane - 1)], rr_sem.at[0])
            mine.wait()

        @pl.when(c != core)
        def _():
            landed(ret.at[pl.ds(core * plane, plane)], rr_sem.at[1])

        lines = plane * CAP
        for i in range(lines // 128):
            first = core * plane + i * (128 // CAP)
            block = ret[first : first + 128 // CAP].astype(F32)
            arr16[first * CAP : first * CAP + 128, :] = block.reshape(128, model).astype(BF16)
        for j in range(model // wide):
            block = arr16[core * lines : (core + 1) * lines, j * wide : (j + 1) * wide]
            picked = [
                jnp.dot(place[k, :, core * lines : (core + 1) * lines], block, preferred_element_type=F32)
                * weights[:, k : k + 1]
                for k in range(2)
            ]
            yield pl.ds(j * wide, wide), picked[0] + picked[1]

    for at, value in take(0):
        total[0:rows_here, at] = value

    sent(res.at[pl.ds(0, n_ep - 1)], rs_sem.at[0])

    for at, value in take(1):
        comb_ref[:, at] = (total[0:rows_here, at] + value).astype(BF16)


def position_tables(count, width):
    quarter = width // 4
    frequency = np.float32(rotary_base) ** (-np.arange(quarter, dtype=np.float32) / np.float32(quarter))
    none = np.zeros((1, quarter))

    def laid(n, first):
        angle = (np.arange(n, dtype=np.float32)[:, None] * frequency).astype(np.float64)
        tables = []
        for value, sign in ((np.cos(angle), 1.0), (np.sin(angle), -1.0)):
            blank = np.broadcast_to(none, value.shape)
            pair = (value, blank) if first else (blank, value)
            tables.append(np.concatenate([sign * pair[0], sign * pair[1], *pair], axis=1))
        return np.stack(tables).astype(np.float32)

    rows = laid(count // GRID_W, True)
    return rows, laid(GRID_W, False)


def on_device(
    queries, keys, values, query_gain, key_gain, routed_rows, mixture_gain,
    expert_index, route_weights, expert_gate, expert_up, expert_down,
):
    length, heads, width = queries.shape
    rows_here, model = routed_rows.shape
    n_tp = lax.axis_size("tp")
    n_ep = lax.axis_size("ep")
    slots = n_ep * CAP
    part = expert_gate.shape[1]
    rows, columns = position_tables(n_ep * length, width)
    rows = jnp.asarray(np.moveaxis(rows.reshape(2, n_ep, length // GRID_W, width), 1, 0))
    vmem = pl.BlockSpec(memory_space=pltpu.VMEM)
    hbm = pl.BlockSpec(memory_space=pl.ANY)
    dma = pltpu.SemaphoreType.DMA
    attended, combined = pl.pallas_call(
        functools.partial(step_kernel, n_tp),
        name="step",
        out_shape=(
            jax.ShapeDtypeStruct((length, heads, width), BF16),
            jax.ShapeDtypeStruct((rows_here, model), BF16),
        ),
        in_specs=[hbm] * 14,
        out_specs=(vmem, vmem),
        scratch_shapes=[
            pltpu.VMEM((length, heads, width), BF16),
            pltpu.VMEM((length, width), BF16),
            pltpu.VMEM((length, width), BF16),
            pltpu.VMEM((rows_here, model), BF16),
            pltpu.VMEM((2, length // GRID_W, width), F32),
            pltpu.VMEM((2, GRID_W, width), F32),
            pltpu.VMEM((1, width), F32),
            pltpu.VMEM((1, width), F32),
            pltpu.VMEM((1, model), F32),
            pltpu.VMEM((2, rows_here), jnp.int32),
            pltpu.VMEM((2, rows_here), F32),
            pltpu.VMEM((NC, NY, NZ, 2 * length, width), BF16),
            pltpu.VMEM((n_tp, 3, part, model), BF16),
            pltpu.VMEM((n_ep, CAP, model), BF16),
            pltpu.VMEM((n_ep, CAP, model), BF16),
            pltpu.VMEM((slots, model), BF16),
            pltpu.VMEM((slots, model), F32),
            pltpu.VMEM((slots, part), BF16),
            pltpu.VMEM((n_ep, CAP, model), BF16),
            pltpu.VMEM((n_ep, CAP, model), BF16),
            pltpu.VMEM((width, heads * length), BF16),
            pltpu.VMEM((width, heads * length), F32),
            pltpu.VMEM((8, heads * length), F32),
            pltpu.VMEM((slots, rows_here), BF16),
            pltpu.VMEM((2, rows_here, slots), BF16),
            dma((11,)),
            dma((3,)),
            dma((2,)),
            dma((4,)),
            dma((9,)),
            dma((1,)),
            dma((7,)),
            dma((1,)),
            dma((4,)),
            dma((1,)),
            dma((NY,)),
            dma((1,)),
            dma((4,)),
            dma((1,)),
            dma((2,)),
            pltpu.SemaphoreType.REGULAR,
        ],
        compiler_params=pltpu.CompilerParams(
            collective_id=0, has_side_effects=True, vmem_limit_bytes=44 * 1024 * 1024
        ),
    )(
        *(
            pltpu.with_memory_space_constraint(array, pltpu.HBM)
            for array in (
                queries, keys.reshape(length, width), values.reshape(length, width), routed_rows,
                rows, jnp.asarray(columns), expert_gate, expert_up, expert_down,
                query_gain.reshape(1, width), key_gain.reshape(1, width), mixture_gain.reshape(1, model),
                expert_index.T, route_weights.T,
            )
        ),
    )
    return attended, combined


def solution(mesh):
    assert dict(mesh.shape) == {"ep": NZ * NY * NC, "tp": 4}
    placed = (
        P("ep", "tp", None),
        P("ep", "tp", None),
        P("ep", "tp", None),
        P(),
        P(),
        P(("ep", "tp"), None),
        P(),
        P(("ep", "tp"), None),
        P(("ep", "tp"), None),
        P("ep", "tp", None),
        P("ep", "tp", None),
        P("ep", "tp", None),
    )
    return jax.shard_map(
        on_device,
        mesh=mesh,
        in_specs=placed,
        out_specs=(P("ep", "tp", None), P(("ep", "tp"), None)),
        check_vma=False,
    )
```

```python
import functools

import jax
import jax.numpy as jnp
import numpy as np
from jax import lax
from jax.experimental import pallas as pl
from jax.experimental.pallas import tpu as pltpu
from jax.sharding import PartitionSpec as P

GROUPS = 4
GRID_W = 64
NZ, NY, NC = 8, 4, 2
CAP = 8
LOG2E = 1.4426950408889634

epsilon = 1e-06
rotary_base = 10000.0
floor_value = -1e30

F32 = jnp.float32
BF16 = jnp.bfloat16


def rms(values_f, gain):
    mean = jnp.mean(values_f * values_f, axis=-1, keepdims=True)
    return values_f * lax.rsqrt(mean + epsilon) * gain


def step_kernel(
    n_tp,
    q_hbm, k_hbm, v_hbm, rows_hbm, row_hbm, col_hbm, gate_ref, up_ref, down_ref,
    qg_hbm, kg_hbm, mg_hbm, ei_hbm, rw_hbm,
    att_ref, comb_ref,
    q_ref, k_ref, v_ref, rows_ref, row_ref, col_ref,
    qg_ref, kg_ref, mg_ref, ei_ref, rw_ref,
    kv, wbuf, out, arr, arr16, total, hid, res, ret, qt, acc, stat, dmat, place,
    in_sem, loc_sem, own_sem, ws_sem, wr_sem, zs_sem, zr_sem, ys_sem, yr_sem, cs_sem, cr_sem,
    ds_sem, dr_sem, rs_sem, rr_sem, go_sem,
):
    me = lax.axis_index("ep")
    t = lax.axis_index("tp")
    z, y, c = me // (NY * NC), (me // NC) % NY, me % NC
    n_ep = NZ * NY * NC
    plane = NZ * NY

    def ep_of(zz, yy, cc):
        return zz * (NY * NC) + yy * NC + cc

    def line(ep):
        return (ep % NC) * plane + ep // NC

    def remote(src, dst, s_sem, r_sem, ep, tp):
        return pltpu.make_async_remote_copy(
            src_ref=src, dst_ref=dst, send_sem=s_sem, recv_sem=r_sem,
            device_id=(ep, tp), device_id_type=pl.DeviceIdType.MESH,
        )

    def sent(ref, sem):
        remote(ref, ref, sem, sem, partner, t).wait_send()

    def landed(ref, sem):
        remote(ref, ref, sem, sem, partner, t).wait_recv()

    partner = ep_of(z, y, (c + 1) % NC)
    t_next, t_prev = (t + 1) % n_tp, (t + n_tp - 1) % n_tp

    barrier = pltpu.get_barrier_semaphore()
    for peer in (t_next, t_prev):
        pl.semaphore_signal(barrier, inc=1, device_id=(me, peer), device_id_type=pl.DeviceIdType.MESH)

    z_at = [(z + dz) % NZ for dz in range(NZ)]
    y_at = [(y + dy) % NY for dy in range(NY)]
    for dy in (2, 1, 3, 0):
        for dz in (4, 3, 5, 2, 6, 1, 7, 0):
            for dc in range(NC):
                if dz + dy + dc > 0:
                    peer = ep_of(z_at[dz], y_at[dy], (c + dc) % NC)
                    pl.semaphore_signal(barrier, inc=1, device_id=(peer, t), device_id_type=pl.DeviceIdType.MESH)

    half = wbuf.shape[2] // 2
    srcs = (gate_ref, up_ref, down_ref)
    reads = [
        pltpu.make_async_copy(src, dst, in_sem.at[i])
        for i, (src, dst) in enumerate(
            (
                (k_hbm, k_ref), (v_hbm, v_ref), (row_hbm.at[me], row_ref), (col_hbm, col_ref),
                (rows_hbm, rows_ref), (q_hbm, q_ref),
                (kg_hbm, kg_ref), (ei_hbm, ei_ref), (mg_hbm, mg_ref), (qg_hbm, qg_ref), (rw_hbm, rw_ref),
            )
        )
    ]
    for read in reads:
        read.start()

    def w_local(p):
        return pltpu.make_async_copy(srcs[p].at[0], wbuf.at[t, p], loc_sem.at[p])

    pl.semaphore_wait(barrier, n_ep - 1 + 2)

    def w_copy(d, stage, p):
        to = t_next if d == 0 else t_prev
        part = pl.ds(0, half) if (d == 0) != (stage == 1) else pl.ds(half, half)
        sems = (
            ws_sem.at[p if stage == 2 else 3],
            wr_sem.at[(3 * d + p, 6, 7 + p // 2)[stage]],
        )
        if stage < 2:
            return remote(srcs[p].at[0, part], wbuf.at[t, p, part], *sems, me, to)
        held = t_prev if d == 0 else t_next
        return remote(wbuf.at[held, p, part], wbuf.at[held, p, part], *sems, me, to)

    def each_w(stage, act):
        for p in range(3):
            for d in range(2):
                act(w_copy(d, stage, p))

    def start_weights():
        for stage in range(2):
            each_w(stage, lambda copy: copy.start())

    def forward_weights():
        for p in range(3):
            for d in range(2):
                w_copy(d, 0, p).wait_recv()
                w_copy(d, 2, p).start()

    @pl.when(c == 0)
    def _():
        start_weights()

    for p in range(3):
        w_local(p).start()

    for read in reads[:4] + reads[6:8]:
        read.wait()
    length, width = k_ref.shape
    lines = row_ref.shape[1]
    tables = [
        (row_ref[i][:, None, :] + col_ref[i][None, :, :]).reshape(length, width) for i in range(2)
    ]

    def turn(x, gain):
        n = rms(x.astype(F32), gain)
        return (n * tables[0] + pltpu.roll(n, width // 2, 1) * tables[1]).astype(BF16)

    kv[c, y, z, 0:length, :] = turn(k_ref[...], kg_ref[...])
    v_t = v_ref[...].astype(F32).T.astype(BF16)
    for j in range(length // width):
        kv[c, y, z, length + j * width : length + (j + 1) * width, :] = v_t[:, j * width : (j + 1) * width]

    def z_copy(j):
        step, back = {1: (1, 0), 2: (1, 1), 3: (1, 2), 4: (1, 3), 7: (-1, 0), 6: (-1, -1), 5: (-1, -2), 0: (-1, -3)}[j]
        held = (z - back + NZ) % NZ
        piece = kv.at[c, y, held]
        if j == 4:
            piece = kv.at[c, y, held, pl.ds(0, length)]
        if j == 0:
            piece = kv.at[c, y, held, pl.ds(length, length)]
        return remote(piece, piece, zs_sem.at[0], zr_sem.at[{1: 1, 7: 2, 2: 3, 6: 4, 3: 5, 5: 6}.get(j, 0)], ep_of((z + step + NZ) % NZ, y, c), t)

    rows_here, model = rows_ref.shape
    pad = jnp.zeros((6, rows_here), F32)
    ids = jnp.concatenate([ei_ref[...].astype(F32), pad], axis=0).T
    lanes = lax.broadcasted_iota(jnp.int32, (rows_here, n_ep), 1).astype(F32)
    hot = [(ids[:, k : k + 1] == lanes).astype(F32) for k in range(2)]
    above = (
        lax.broadcasted_iota(jnp.int32, (rows_here, rows_here), 1)
        < lax.broadcasted_iota(jnp.int32, (rows_here, rows_here), 0)
    ).astype(F32).astype(BF16)
    earlier = jnp.dot(above, (hot[0] + hot[1]).astype(BF16), preferred_element_type=F32)
    slots = lax.broadcasted_iota(jnp.int32, (rows_here, n_ep * CAP), 1).astype(F32)
    picks = []
    for k in range(2):
        upper = jnp.floor(ids[:, k : k + 1] * (1.0 / NC))
        row = (ids[:, k : k + 1] - upper * NC) * plane + upper
        at = row * CAP + jnp.sum(earlier * hot[k], axis=1, keepdims=True)
        pick = (at == slots).astype(F32)
        place[k] = pick.astype(BF16)
        picks.append(pick)
    dmat[...] = (picks[0] + picks[1]).T.astype(BF16)

    for j in (1, 7):
        z_copy(j).start()

    reads[4].wait()
    reads[8].wait()
    arr16[0:rows_here, :] = rms(rows_ref[...].astype(F32), mg_ref[...]).astype(BF16)

    @pl.loop(0, n_ep * CAP // 128)
    def _(i):
        block = jnp.dot(
            dmat[pl.ds(i * 128, 128), :], arr16[0:rows_here, :], preferred_element_type=F32
        )
        out[pl.ds(i * (128 // CAP), 128 // CAP)] = block.reshape(128 // CAP, CAP, model).astype(BF16)

    def alternate(i):
        side = 1 - 2 * (i % 2)
        return (NZ // 2 + side * ((i + 1) // 2) + NZ) % NZ

    def beyond(i):
        return alternate(i) * (1 - i // 5)

    def send_row(core, dz, dy):
        dc = (c + core) % NC
        row = (z + dz) % NZ * NY + y_at[dy]
        k = dc * plane + dy * NZ + dz
        copy = remote(
            out.at[core * plane + row], arr.at[k], ds_sem.at[0], dr_sem.at[2 * dc + dy // 2], row * NC + core, t
        )
        if dy > 0:
            copy.start()
        else:
            pl.when(k > 0)(copy.start)

    own = pltpu.make_async_copy(out.at[line(me)], arr.at[0], own_sem.at[0])
    own.start()
    fill = [(core, dy) for core in range(NC) for dy in range(NY)]
    hops = ((1, 7), (2, 6), (3, 5), (4, 0))
    for i in range(4):
        if i > 0:
            for d in range(2):
                z_copy(hops[i - 1][d]).wait_recv()
                z_copy(hops[i][d]).start()
        for core, dy in fill[3 * i : 3 * (i + 1)] if i < 3 else fill[3 * 3 :]:
            send_row(core, 1, dy)
            send_row(core, NZ - 1, dy)

    def dispatch(core):
        for dy in range(NY):

            @pl.loop(0, NZ - 2)
            def _(i):
                dz = beyond(i)
                send_row(core, dz, dy)

    dispatch(0)
    dispatch(1)

    reads[5].wait()
    reads[9].wait()
    q_f = q_ref[...].astype(F32)
    for h in range(q_ref.shape[1]):
        turned = turn(q_f[:, h, :], qg_ref[...])
        qt[:, h * length : (h + 1) * length] = turned.astype(F32).T.astype(BF16)

    zh = NZ // 2

    def y_copy(d, stage):
        to = (y + 1) % NY if d == 0 else (y + NY - 1) % NY
        part = pl.ds(0, zh) if (d == 0) != (stage == 1) else pl.ds(zh, zh)
        held = y if stage < 2 else ((y + NY - 1) % NY if d == 0 else (y + 1) % NY)
        piece = kv.at[c, held, part]
        return remote(piece, piece, ys_sem.at[0], yr_sem.at[d if stage == 0 else stage + 1], ep_of(z, to, c), t)

    def c_copy(dy):
        piece = kv.at[c, (y + dy) % NY]
        return remote(piece, piece, cs_sem.at[0], cr_sem.at[dy], partner, t)

    def start_y():
        landed(kv.at[c, y, 0], zr_sem.at[0])
        for stage in range(2):
            for d in range(2):
                y_copy(d, stage).start()
        c_copy(0).start()

    def forward_y():
        for d in range(2):
            y_copy(d, 0).wait_recv()
            y_copy(d, 2).start()

    def near_y():
        landed(kv.at[c, 0], yr_sem.at[2])
        c_copy(1).start()
        c_copy(3).start()

    def far_y():
        landed(kv.at[c, 0], yr_sem.at[3])
        c_copy(2).start()

    step = 256
    chunks = n_ep * CAP // step
    contract = (((1,), (1,)), ((), ()))

    def hidden_of(x, q):
        g = lax.dot_general(x, wbuf[q, 0], contract, preferred_element_type=F32)
        u = lax.dot_general(x, wbuf[q, 1], contract, preferred_element_type=F32)
        return (g / (1.0 + jnp.exp(-g)) * u).astype(BF16)

    def expert(q, i):
        at = pl.ds(i * step, step)
        part = jnp.dot(hidden_of(arr16[at, :], q), wbuf[q, 2], preferred_element_type=F32)
        return at, part.astype(BF16).astype(F32)

    def first_part():
        own.wait()
        for p in range(3):
            w_local(p).wait()
        group = 128 // CAP

        for i in range(n_ep // group):
            low = max(i * group, 1)
            landed(arr.at[pl.ds(low, (i + 1) * group - low)], dr_sem.at[i])
            block = arr[i * group : (i + 1) * group].astype(F32)
            arr16[i * 128 : (i + 1) * 128, :] = block.reshape(128, model).astype(BF16)

        @pl.loop(0, chunks)
        def _(i):
            at, part = expert(t, i)
            total[at, :] = part

    def add_part(held):
        @pl.loop(0, chunks)
        def _(i):
            at, part = expert(held, i)
            total[at, :] = total[at, :] + part

    mine = pltpu.make_async_copy(res.at[0], ret.at[line(me)], own_sem.at[1])

    def last_part():
        last = (t + 2) % n_tp
        per = step // CAP // 2
        landed(wbuf.at[0, pl.ds(0, 2)], wr_sem.at[7])

        @pl.loop(0, chunks)
        def _(i):
            at = pl.ds(i * step, step)
            hid[at, :] = hidden_of(arr16[at, :], last)

        landed(wbuf.at[0, 2], wr_sem.at[8])

        piece = step // 2

        @pl.loop(0, 2 * chunks)
        def _(i):
            at = pl.ds(i * piece, piece)
            part = jnp.dot(hid[at, :], wbuf[last, 2], preferred_element_type=F32).astype(BF16).astype(F32)
            block = (total[at, :] + part).astype(BF16).astype(F32)
            res[pl.ds(i * per, per)] = block.reshape(per, CAP, model).astype(BF16)

            dc = i // 2
            core = (c + dc) % NC

            for pair in range(2):
                dy = i % 2 * 2 + pair

                @pl.loop(0, NZ)
                def _(j):
                    dz = alternate(j)
                    row = (z + NZ - dz) % NZ * NY + (y + NY - dy) % NY
                    k = dc * plane + dy * NZ + dz
                    copy = remote(
                        res.at[k], ret.at[line(me)], rs_sem.at[0], rr_sem.at[dc], row * NC + core, t
                    )
                    pl.when(k > 0)(copy.start)

        mine.start()

    cols = qt.shape[1]
    factor = width ** (-0.5) * LOG2E
    stat[0:1, :] = jnp.full((1, cols), floor_value, F32)
    stat[1:2, :] = jnp.zeros((1, cols), F32)
    acc[...] = jnp.zeros_like(acc)

    def one_block(cc, yy, zz):
        k_block = kv[cc, yy, zz, 0:length, :]
        v_block = jnp.concatenate(
            [kv[cc, yy, zz, length + j * width : length + (j + 1) * width, :] for j in range(length // width)],
            axis=1,
        )
        s = jnp.dot(k_block, qt[...], preferred_element_type=F32)
        m_b = jnp.max(s, axis=0, keepdims=True)
        p = jnp.exp2((s - m_b) * factor)
        l_b = jnp.sum(p, axis=0, keepdims=True)
        a_b = jnp.dot(v_block, p.astype(BF16), preferred_element_type=F32)
        return m_b, l_b, a_b

    def attend(dy, core):
        yy = (y + dy) % NY

        @pl.loop(0, zh)
        def _(zz):
            cc = (c + core) % NC
            m_0, l_0, a_0 = one_block(cc, yy, 2 * zz)
            m_1, l_1, a_1 = one_block(cc, yy, 2 * zz + 1)
            m_old = stat[0:1, :]
            top = jnp.maximum(jnp.maximum(m_0, m_1), m_old)
            keep = jnp.exp2((m_old - top) * factor)
            n_0 = jnp.exp2((m_0 - top) * factor)
            n_1 = jnp.exp2((m_1 - top) * factor)
            stat[0:1, :] = top
            stat[1:2, :] = stat[1:2, :] * keep + l_0 * n_0 + l_1 * n_1
            acc[...] = acc[...] * keep + a_0 * n_0 + a_1 * n_1

    @pl.when(c == 0)
    def _():
        forward_weights()
        start_y()
        attend(0, 0)
        c_copy(0).wait_recv()
        attend(0, 1)
        for p in range(2):
            sent(wbuf.at[0, p], ws_sem.at[p])
        pl.semaphore_signal(go_sem, inc=1, device_id=(partner, t), device_id_type=pl.DeviceIdType.MESH)
        forward_y()
        first_part()
        landed(wbuf.at[0], wr_sem.at[6])
        add_part(t_prev)
        add_part(t_next)
        last_part()
        near_y()
        for dy in (1, 3):
            attend(dy, 0)
        for dy in (1, 3):
            c_copy(dy).wait_recv()
            attend(dy, 1)
        far_y()
        attend(2, 0)
        c_copy(2).wait_recv()
        attend(2, 1)

    @pl.when(c == 1)
    def _():
        start_y()
        attend(0, 0)
        c_copy(0).wait_recv()
        attend(0, 1)
        forward_y()
        pl.semaphore_wait(go_sem, 1)
        start_weights()
        near_y()
        attend(1, 0)
        forward_weights()
        attend(3, 0)
        first_part()
        landed(wbuf.at[0], wr_sem.at[6])
        add_part(t_prev)
        add_part(t_next)
        far_y()
        attend(2, 0)
        last_part()
        for dy in (1, 3, 2):
            c_copy(dy).wait_recv()
            attend(dy, 1)
        for p in range(2):
            sent(wbuf.at[0, p], ws_sem.at[p])

    done = acc[...] / stat[1:2, :]
    heads = [done[:, h * length : (h + 1) * length].T for h in range(cols // length)]
    att_ref[...] = jnp.stack(heads, axis=1).astype(BF16)

    sent(wbuf.at[pl.ds(0, 2)], ws_sem.at[3])
    sent(wbuf.at[0, 2], ws_sem.at[2])
    sent(kv.at[c, y, pl.ds(0, NZ - 1)], zs_sem.at[0])
    sent(kv.at[c, pl.ds(0, NY - 1)], ys_sem.at[0])
    sent(kv.at[c], cs_sem.at[0])
    sent(out.at[pl.ds(0, n_ep - 1)], ds_sem.at[0])

    reads[10].wait()
    weights = jnp.concatenate([rw_ref[...], pad], axis=0).T
    wide = 512

    def take(core):
        @pl.when(c == core)
        def _():
            landed(ret.at[pl.ds(core * plane, plane - 1)], rr_sem.at[0])
            mine.wait()

        @pl.when(c != core)
        def _():
            landed(ret.at[pl.ds(core * plane, plane)], rr_sem.at[1])

        lines = plane * CAP
        both = place[:, :, core * lines : (core + 1) * lines].reshape(2 * rows_here, lines)
        for j in range(model // wide):
            at = pl.ds(j * wide, wide)
            block = ret[core * plane : (core + 1) * plane, :, at].astype(F32)
            picked = jnp.dot(both, block.reshape(lines, wide).astype(BF16), preferred_element_type=F32)
            yield at, picked[:rows_here] * weights[:, 0:1] + picked[rows_here:] * weights[:, 1:2]

    for at, value in take(0):
        total[0:rows_here, at] = value

    sent(res.at[pl.ds(0, n_ep - 1)], rs_sem.at[0])

    for at, value in take(1):
        comb_ref[:, at] = (total[0:rows_here, at] + value).astype(BF16)


def position_tables(count, width):
    quarter = width // 4
    frequency = np.float32(rotary_base) ** (-np.arange(quarter, dtype=np.float32) / np.float32(quarter))
    none = np.zeros((1, quarter))

    def laid(n, first):
        angle = (np.arange(n, dtype=np.float32)[:, None] * frequency).astype(np.float64)
        tables = []
        for value, sign in ((np.cos(angle), 1.0), (np.sin(angle), -1.0)):
            blank = np.broadcast_to(none, value.shape)
            pair = (value, blank) if first else (blank, value)
            tables.append(np.concatenate([sign * pair[0], sign * pair[1], *pair], axis=1))
        return np.stack(tables).astype(np.float32)

    rows = laid(count // GRID_W, True)
    return rows, laid(GRID_W, False)


def on_device(
    queries, keys, values, query_gain, key_gain, routed_rows, mixture_gain,
    expert_index, route_weights, expert_gate, expert_up, expert_down,
):
    length, heads, width = queries.shape
    rows_here, model = routed_rows.shape
    n_tp = lax.axis_size("tp")
    n_ep = lax.axis_size("ep")
    slots = n_ep * CAP
    part = expert_gate.shape[1]
    rows, columns = position_tables(n_ep * length, width)
    rows = jnp.asarray(np.moveaxis(rows.reshape(2, n_ep, length // GRID_W, width), 1, 0))
    vmem = pl.BlockSpec(memory_space=pltpu.VMEM)
    hbm = pl.BlockSpec(memory_space=pl.ANY)
    dma = pltpu.SemaphoreType.DMA
    attended, combined = pl.pallas_call(
        functools.partial(step_kernel, n_tp),
        name="step",
        out_shape=(
            jax.ShapeDtypeStruct((length, heads, width), BF16),
            jax.ShapeDtypeStruct((rows_here, model), BF16),
        ),
        in_specs=[hbm] * 14,
        out_specs=(vmem, vmem),
        scratch_shapes=[
            pltpu.VMEM((length, heads, width), BF16),
            pltpu.VMEM((length, width), BF16),
            pltpu.VMEM((length, width), BF16),
            pltpu.VMEM((rows_here, model), BF16),
            pltpu.VMEM((2, length // GRID_W, width), F32),
            pltpu.VMEM((2, GRID_W, width), F32),
            pltpu.VMEM((1, width), F32),
            pltpu.VMEM((1, width), F32),
            pltpu.VMEM((1, model), F32),
            pltpu.VMEM((2, rows_here), jnp.int32),
            pltpu.VMEM((2, rows_here), F32),
            pltpu.VMEM((NC, NY, NZ, 2 * length, width), BF16),
            pltpu.VMEM((n_tp, 3, part, model), BF16),
            pltpu.VMEM((n_ep, CAP, model), BF16),
            pltpu.VMEM((n_ep, CAP, model), BF16),
            pltpu.VMEM((slots, model), BF16),
            pltpu.VMEM((slots, model), F32),
            pltpu.VMEM((slots, part), BF16),
            pltpu.VMEM((n_ep, CAP, model), BF16),
            pltpu.VMEM((n_ep, CAP, model), BF16),
            pltpu.VMEM((width, heads * length), BF16),
            pltpu.VMEM((width, heads * length), F32),
            pltpu.VMEM((8, heads * length), F32),
            pltpu.VMEM((slots, rows_here), BF16),
            pltpu.VMEM((2, rows_here, slots), BF16),
            dma((11,)),
            dma((3,)),
            dma((2,)),
            dma((4,)),
            dma((9,)),
            dma((1,)),
            dma((7,)),
            dma((1,)),
            dma((4,)),
            dma((1,)),
            dma((NY,)),
            dma((1,)),
            dma((4,)),
            dma((1,)),
            dma((2,)),
            pltpu.SemaphoreType.REGULAR,
        ],
        compiler_params=pltpu.CompilerParams(
            collective_id=0, has_side_effects=True, vmem_limit_bytes=44 * 1024 * 1024
        ),
    )(
        *(
            pltpu.with_memory_space_constraint(array, pltpu.HBM)
            for array in (
                queries, keys.reshape(length, width), values.reshape(length, width), routed_rows,
                rows, jnp.asarray(columns), expert_gate, expert_up, expert_down,
                query_gain.reshape(1, width), key_gain.reshape(1, width), mixture_gain.reshape(1, model),
                expert_index.T, route_weights.T,
            )
        ),
    )
    return attended, combined


def solution(mesh):
    assert dict(mesh.shape) == {"ep": NZ * NY * NC, "tp": 4}
    placed = (
        P("ep", "tp", None),
        P("ep", "tp", None),
        P("ep", "tp", None),
        P(),
        P(),
        P(("ep", "tp"), None),
        P(),
        P(("ep", "tp"), None),
        P(("ep", "tp"), None),
        P("ep", "tp", None),
        P("ep", "tp", None),
        P("ep", "tp", None),
    )
    return jax.shard_map(
        on_device,
        mesh=mesh,
        in_specs=placed,
        out_specs=(P("ep", "tp", None), P(("ep", "tp"), None)),
        check_vma=False,
    )
```
